768 devices in a mesh: sp: 16 (over y, core), dp: 48 (over z, x).
Axes of the slice: x: 4, y: 8, z: 12, core: 2. Of those that a mesh axis runs over, the one named last changes fastest.
Arguments:
- standardized_block_source: bfloat16 [96, 1024, 2064], P('dp', 'sp'), may hold values from -6 to 6
- forgetting_narrowing_matrix: bfloat16 [2064, 32], P('dp'), may hold values from -0.125 to 0.125
- forgetting_widening_matrix: bfloat16 [32, 1024], replicated, may hold values from -1 to 1
- forgetting_offset_vector: float32 [1024], replicated, may hold values from -1.5 to 6.5
- probe_vectors: bfloat16 [768, 1024, 128], P(('dp', 'sp')), may hold values from -6 to 6
- address_vectors: bfloat16 [768, 1024, 128], P(('dp', 'sp')), may hold values from -6 to 6
- payload_vectors: bfloat16 [768, 1024, 256], P(('dp', 'sp')), may hold values from -6 to 6
- extra_channel_forgetting: float32 [768, 1024], P(('dp', 'sp')), may hold values from -2.1 to 0
- blender_result_adjoint: bfloat16 [96, 1024, 2048], P('dp', 'sp'), may hold values from -0.29882812 to 0.29882812
Outputs:
- grad_queries: bfloat16 [96, 1024, 1024], P('dp', 'sp')
- grad_keys: bfloat16 [96, 1024, 1024], P('dp', 'sp')
- grad_values: bfloat16 [96, 1024, 2048], P('dp', 'sp')
- grad_input: bfloat16 [96, 1024, 2064], P('dp', 'sp')
- grad_gate_down: float32 [2064, 32], P('dp')
- grad_gate_up: float32 [32, 1024], replicated
- grad_gate_bias: float32 [1024], replicated
The draws below stay inside these ranges and needn't reach their ends.
All inputs are finite; a program needn't handle non-finite values.
Results may differ from the reference program's by a relative error of at most 0.0069.
Values may be sent and summed in bfloat16 or wider, within the bound.
No kernel may reach another device: no remote copies, remote signals or barrier semaphores. Data moves between devices by JAX's collectives and lax.ppermute only.
A program may use at most 32 MiB of HBM per device.

```python
import jax
import jax.numpy as jnp
from jax import lax

D = 2064
HEADS = 8
ADDRESS_WIDTH = 128
PAYLOAD_WIDTH = 256
RANK = 32
BLOCK = 64
LEN = 1024
BATCH = 96
KD = 1024
VD = 2048


def draw_forgetting_offset_vector(key, part):
    pick_key, level_key, jitter_key = jax.random.split(jax.random.fold_in(key, 11), 3)
    slow_share = 0.5
    slow_heads = jax.random.uniform(pick_key, (HEADS,)) < slow_share
    slow_level = jax.random.uniform(level_key, (HEADS,), minval=4.5, maxval=6.0)
    fast_level = jax.random.uniform(jax.random.fold_in(level_key, 1), (HEADS,), minval=-1.0, maxval=0.5)
    levels = jnp.where(slow_heads, slow_level, fast_level)
    jitter = jax.random.uniform(jitter_key, (HEADS, ADDRESS_WIDTH), minval=-0.5, maxval=0.5)
    return (levels[:, None] + jitter).reshape(HEADS * ADDRESS_WIDTH).astype(jnp.float32)


def draw_extra_channel_forgetting(key, part):
    place_key, loss_key = jax.random.split(jax.random.fold_in(key, 23))
    item_rows = BATCH * HEADS
    positions = jax.random.randint(place_key, (item_rows, 3, 1), 0, LEN)
    losses = jnp.log(jax.random.uniform(loss_key, (item_rows, 3, 1), minval=0.5, maxval=0.8))
    places = jnp.arange(LEN, dtype=jnp.int32)[None, None, :]
    return jnp.sum(jnp.where(places == positions, losses, 0.0), axis=1).astype(jnp.float32)


def strengthened(values, own_key, source, target, shards_of, factor):
    def block_of(position):
        return (jnp.arange(values.shape[position]) // (values.shape[position] // shards_of)).reshape((-1,) + (1,) * (values.ndim - 1 - position))

    first = jax.random.permutation(own_key, shards_of)[block_of(target)]
    second = (block_of(target) + shards_of // 2) % shards_of
    return jnp.where((block_of(source) == first) | (block_of(source) == second), factor * values, values)


def block_levels(key, shape, cuts, low, high):
    def one(position, parts):
        draws = jax.random.uniform(jax.random.fold_in(jax.random.fold_in(key, 6), position), (parts,), jnp.float32, low / len(cuts), high / len(cuts))
        return jnp.repeat(jnp.exp(draws), shape[position] // parts).reshape((-1,) + (1,) * (len(shape) - position - 1))

    loudness = one(*cuts[0])
    for cut in cuts[1:]:
        loudness = loudness * one(*cut)
    return loudness


def gaussian(own_key, extent, width, reach, cuts=(), kind=jnp.bfloat16):
    loudness = block_levels(own_key, extent, cuts, -0.22, 0.18) if cuts else 1.0
    result = jax.random.normal(own_key, extent, jnp.float32) * width * loudness
    return jnp.minimum(jnp.maximum(result, -reach), reach).astype(kind)


def heavy_noise(own_key, shape, width, most, cuts, heavy, kind=jnp.bfloat16):
    values = width * jax.random.normal(own_key, shape, jnp.float32)
    if cuts:
        values = values * block_levels(own_key, shape, cuts, -0.22, 0.18)
    return jnp.clip(strengthened(values, jax.random.fold_in(own_key, 3), *heavy), -most, most).astype(kind)


def setup_inputs(seed: int = 0) -> dict:
    keys = jax.random.split(jax.random.key(seed), 10)
    return {
        "standardized_block_source": heavy_noise(keys[0], (BATCH, LEN, D), 1.0, 6.0, ((0, 48), (1, 16)), (0, 2, 48, 3.25)),
        "forgetting_narrowing_matrix": gaussian(keys[1], (D, RANK), D ** -0.5, 0.125, ((0, 48),)),
        "forgetting_widening_matrix": gaussian(keys[2], (RANK, KD), RANK ** -0.5, 1.0),
        "forgetting_offset_vector": draw_forgetting_offset_vector(jax.random.fold_in(keys[9], 71), 0),
        "probe_vectors": gaussian(keys[4], (BATCH * HEADS, LEN, ADDRESS_WIDTH), 1.0, 6.0, ((0, 768),)),
        "address_vectors": gaussian(keys[5], (BATCH * HEADS, LEN, ADDRESS_WIDTH), 1.0, 6.0, ((0, 768),)),
        "payload_vectors": gaussian(keys[6], (BATCH * HEADS, LEN, PAYLOAD_WIDTH), 1.0, 6.0, ((0, 768),)),
        "extra_channel_forgetting": draw_extra_channel_forgetting(jax.random.fold_in(keys[9], 71), 0),
        "blender_result_adjoint": gaussian(keys[8], (BATCH, LEN, VD), 0.05, 0.29882812, ((0, 48), (1, 16))),
    }


retention_smoothing = 16.0

def head_forward(stream_probe_entries, stream_address_entries, stream_payload_entries, retention_coefficient):
    length, key_width = stream_probe_entries.shape
    value_width = stream_payload_entries.shape[1]
    blocks = length // BLOCK
    scaled = stream_probe_entries * key_width ** (-0.5)
    causal = jnp.tril(jnp.ones((BLOCK, BLOCK), dtype=bool))
    highest = lax.Precision.HIGHEST

    def advance(memory, pieces):
        query_block, key_block, value_block, decay_sums = pieces
        spread = decay_sums[:, None, :] - decay_sums[None, :, :]
        decays = jnp.exp(jnp.where(causal[:, :, None], spread, -jnp.inf))
        scores = jnp.einsum('td,sd,tsd->ts', query_block, key_block, decays, precision=highest)
        within = jnp.dot(scores, value_block, precision=highest)
        carried = jnp.dot(query_block * jnp.exp(decay_sums), memory, precision=highest)
        ending = decay_sums[-1]
        fading = key_block * jnp.exp(ending[None, :] - decay_sums)
        memory = memory * jnp.exp(ending)[:, None] + jnp.dot(fading.T, value_block, precision=highest)
        return (memory, within + carried)

    def blocked(tensor):
        return tensor.reshape(blocks, BLOCK, tensor.shape[1])
    initial = jnp.zeros((key_width, value_width), jnp.float32)
    decay_sums = jnp.cumsum(blocked(retention_coefficient), axis=1)
    _, outputs = lax.scan(jax.checkpoint(advance), initial, (blocked(scaled), blocked(stream_address_entries), blocked(stream_payload_entries), decay_sums))
    return outputs.reshape(length, value_width)

def stream_sensitivities(stream_probe_entries, stream_address_entries, stream_payload_entries, forgetting_logit_values, surplus_retention_loss, result_adjoint):

    def forward(query_in, key_in, value_in, retention_basis_components):
        retention_coefficient = jax.nn.log_sigmoid(retention_basis_components) / retention_smoothing + surplus_retention_loss[:, None]
        return head_forward(query_in, key_in, value_in, retention_coefficient)
    _, pullback = jax.vjp(forward, stream_probe_entries.astype(jnp.float32), stream_address_entries.astype(jnp.float32), stream_payload_entries.astype(jnp.float32), forgetting_logit_values)
    query_grad, key_grad, value_grad, gate_grad = pullback(result_adjoint.astype(jnp.float32))
    return (query_grad.astype(jnp.bfloat16), key_grad.astype(jnp.bfloat16), value_grad.astype(jnp.bfloat16), gate_grad.astype(jnp.bfloat16))

def reference(standardized_block_source, forgetting_narrowing_matrix, forgetting_widening_matrix, forgetting_offset_vector, probe_vectors, address_vectors, payload_vectors, extra_channel_forgetting, blender_result_adjoint):
    batch, length, model_width = standardized_block_source.shape
    flat_input = standardized_block_source.reshape(batch * length, model_width)
    low_rank = jnp.dot(flat_input, forgetting_narrowing_matrix, preferred_element_type=jnp.float32).astype(jnp.bfloat16)
    logit_by_position = jnp.dot(low_rank, forgetting_widening_matrix, preferred_element_type=jnp.float32) + forgetting_offset_vector

    def regroup_into_entries(tensor, columns):
        return tensor.reshape(batch, length, HEADS, columns).transpose(0, 2, 1, 3).reshape(batch * HEADS, length, columns)

    def to_tokens(tensor):
        columns = tensor.shape[2]
        return tensor.reshape(batch, HEADS, length, columns).transpose(0, 2, 1, 3).reshape(batch, length, HEADS * columns)

    def single_sample_entries(pieces):
        return stream_sensitivities(pieces[0], pieces[1], pieces[2], pieces[3], pieces[4], pieces[5])
    weight_sensitivities = lax.map(single_sample_entries, (probe_vectors, address_vectors, payload_vectors, regroup_into_entries(logit_by_position, ADDRESS_WIDTH), extra_channel_forgetting, regroup_into_entries(blender_result_adjoint, PAYLOAD_WIDTH)))
    gate_tokens = to_tokens(weight_sensitivities[3]).reshape(batch * length, HEADS * ADDRESS_WIDTH)
    low_grad = jnp.dot(gate_tokens, forgetting_widening_matrix.T, preferred_element_type=jnp.float32).astype(jnp.bfloat16)
    incoming_sensitivity = jnp.dot(low_grad, forgetting_narrowing_matrix.T, preferred_element_type=jnp.float32).astype(jnp.bfloat16)
    contract = (((0,), (0,)), ((), ()))
    down_grad = lax.dot_general(flat_input, low_grad, contract, preferred_element_type=jnp.float32)
    up_grad = lax.dot_general(low_rank, gate_tokens, contract, preferred_element_type=jnp.float32)
    bias_grad = lax.optimization_barrier(jnp.sum(gate_tokens.astype(jnp.float32), axis=0))
    return (to_tokens(weight_sensitivities[0]), to_tokens(weight_sensitivities[1]), to_tokens(weight_sensitivities[2]), incoming_sensitivity.reshape(batch, length, model_width), down_grad, up_grad, bias_grad)
```

```python
import jax
import jax.numpy as jnp
from jax import lax
from jax.experimental import pallas as pl
from jax.experimental.pallas import tpu as pltpu
from jax.sharding import PartitionSpec as P

HEADS = 8
ADDRESS_WIDTH = 128
PAYLOAD_WIDTH = 256
RANK = 32
BLOCK = 64
SMOOTHING = 16.0
SPAN_LIMIT = 80.0
PACK = 4
f32 = jnp.float32
bf16 = jnp.bfloat16


def mm(a, b, ca=1, cb=0):
    return lax.dot_general(a, b, (((ca,), (cb,)), ((), ())), preferred_element_type=f32)


def two_parts(a):
    hi = a.astype(bf16)
    return hi, (a - hi.astype(f32)).astype(bf16)


def three_parts(a):
    hi = a.astype(bf16)
    return hi, *two_parts(a - hi.astype(f32))


def mixer_kernel(
    came_ref, wu_ref, off_ref, ex_ref, q_ref, k_ref, v_ref,
    goes_ref, bias_ref,
    wbig, parts, b_s, pre_s, qp_s, kf_s, st_s, pt_s, dqi_s, dki_s, x_s, y_s, e_s, gate_s,
):
    blocks = q_ref.shape[0]
    rows = BLOCK // PACK
    lanes = ADDRESS_WIDTH
    scale = ADDRESS_WIDTH ** (-0.5)
    middle = BLOCK // 2

    def do_block(n):
        return jnp.concatenate(
            [came_ref[n, BLOCK * i : BLOCK * (i + 1)] for i in range(PAYLOAD_WIDTH // lanes)],
            axis=1,
        )

    row_id = lax.broadcasted_iota(jnp.int32, (BLOCK, BLOCK), 0)
    col_id = lax.broadcasted_iota(jnp.int32, (BLOCK, BLOCK), 1)

    wbig[...] = jnp.zeros(wbig.shape, bf16)
    for p in range(PACK):
        wbig[RANK * p : RANK * (p + 1), lanes * p : lanes * (p + 1)] = wu_ref[...]
    low = came_ref[:, 2 * BLOCK :].reshape(blocks * rows, lanes)
    raw = mm(low, wbig[...])
    offs = off_ref[...]
    for n in range(blocks):
        pre = (
            jnp.concatenate(
                [
                    raw[rows * n : rows * (n + 1), lanes * p : lanes * (p + 1)]
                    for p in range(PACK)
                ],
                axis=0,
            )
            + offs
        )
        pre_s[n] = pre
        decay = (jnp.minimum(pre, 0.0) - jnp.log1p(jnp.exp(-jnp.abs(pre)))) * (
            1.0 / SMOOTHING
        ) + ex_ref[:, n : n + 1]
        for i, part in enumerate(three_parts(decay)):
            parts[BLOCK * i : BLOCK * (i + 1), lanes * n : lanes * (n + 1)] = part
    lower = (row_id >= col_id).astype(bf16)
    sums = mm(jnp.concatenate([lower] * 3, axis=1), parts[: 3 * BLOCK])
    span = jnp.zeros((1, lanes), f32)
    for n in range(blocks):
        b = sums[:, lanes * n : lanes * (n + 1)]
        b_s[n] = b
        centre = b[middle : middle + 1]
        span = jnp.maximum(span, jnp.maximum(b[:1] - centre, centre - b[BLOCK - 1 :]))
    narrow = jnp.max(span) < SPAN_LIMIT

    @pl.when(narrow)
    def _():
        def within(n, carry):
            b = b_s[n]
            centre = b[middle : middle + 1]
            lift = jnp.exp(b - centre)
            drop = jnp.exp(centre - b)
            qc = (q_ref[n].astype(f32) * scale * lift).astype(bf16)
            kc = (k_ref[n].astype(f32) * drop).astype(bf16)
            do = do_block(n)
            v = v_ref[n]
            pt_s[n] = jnp.where(row_id <= col_id, mm(kc, qc, 1, 1), 0.0).astype(bf16)
            dp = jnp.where(row_id >= col_id, mm(do, v, 1, 1), 0.0).astype(bf16)
            dq = mm(dp, kc)
            dk = mm(dp, qc, 0, 0)
            x_s[n] = dq * qc.astype(f32) - dk * kc.astype(f32)
            dqi_s[n] = dq * lift
            dki_s[n] = dk * drop
            return carry

        lax.fori_loop(0, blocks, within, 0, unroll=4)

    @pl.when(jnp.logical_not(narrow))
    def _():
        def within(n, carry):
            b = b_s[n]
            q = q_ref[n].astype(f32) * scale
            dp = mm(do_block(n), v_ref[n], 1, 1)
            at = lax.broadcasted_iota(jnp.int32, (BLOCK, 1), 0)
            dqi_s[n] = jnp.zeros((BLOCK, lanes), f32)
            x_s[n] = jnp.zeros((BLOCK, lanes), f32)

            def one(s, scores):
                here = at == s
                b_row = jnp.sum(jnp.where(here, b, 0.0), axis=0, keepdims=True)
                k_row = jnp.sum(
                    jnp.where(here, k_ref[n].astype(f32), 0.0), axis=0, keepdims=True
                )
                decay = jnp.where(at >= s, jnp.exp(jnp.minimum(b - b_row, 0.0)), 0.0)
                dp_col = jnp.sum(jnp.where(col_id == s, dp, 0.0), axis=1, keepdims=True)
                qd = q * decay
                column = jnp.sum(qd * k_row, axis=1, keepdims=True)
                dq = dp_col * decay * k_row
                dk_row = jnp.sum(dp_col * qd, axis=0, keepdims=True)
                dqi_s[n] = dqi_s[n] + dq
                dki_s[n] = jnp.where(here, dk_row, dki_s[n])
                x_s[n] = x_s[n] + q * dq - jnp.where(here, dk_row * k_row, 0.0)
                return scores + jnp.where(col_id == s, column, 0.0)

            scores = lax.fori_loop(0, BLOCK, one, jnp.zeros((BLOCK, BLOCK), f32))
            pt_s[n] = scores.T.astype(bf16)
            return carry

        lax.fori_loop(0, blocks, within, 0)

    def forward(n, state):
        b = b_s[n]
        last = b[BLOCK - 1 :]
        grow = jnp.exp(b)
        qp = (q_ref[n].astype(f32) * scale * grow).astype(bf16)
        kf = (k_ref[n].astype(f32) * jnp.exp(last - b)).astype(bf16)
        qp_s[n] = qp
        kf_s[n] = kf
        st_s[n] = state
        dq = mm(do_block(n), state.astype(bf16))
        x_s[n] = x_s[n] + qp.astype(f32) * dq
        goes_ref[n, :BLOCK] = ((dqi_s[n] + dq * grow) * scale).astype(bf16)
        return state * jnp.exp(last) + mm(v_ref[n], kf, 0, 0)

    zero = jnp.zeros((PAYLOAD_WIDTH, lanes), f32)
    lax.fori_loop(0, blocks, forward, zero, unroll=4)

    def backward(i, dstate):
        n = blocks - 1 - i
        b = b_s[n]
        last = b[BLOCK - 1 :]
        do = do_block(n)
        ds = dstate.astype(bf16)
        kf = kf_s[n]
        dk = mm(v_ref[n], ds)
        goes_ref[n, BLOCK : 2 * BLOCK] = (dki_s[n] + dk * jnp.exp(last - b)).astype(bf16)
        dv = (mm(pt_s[n], do) + mm(kf, ds, 1, 1)).astype(bf16)
        goes_ref[n, 2 * BLOCK : 3 * BLOCK] = dv[:, :lanes]
        goes_ref[n, 3 * BLOCK : 4 * BLOCK] = dv[:, lanes:]
        y_s[n] = kf.astype(f32) * dk
        fade = jnp.exp(last)
        e_s[n] = fade * jnp.sum(st_s[n] * dstate, axis=0, keepdims=True)
        return dstate * fade + mm(do, qp_s[n], 0, 0)

    lax.fori_loop(0, blocks, backward, zero, unroll=4)

    for n in range(blocks):
        for i, part in enumerate(three_parts(x_s[n])):
            parts[BLOCK * i : BLOCK * (i + 1), lanes * n : lanes * (n + 1)] = part
        for i, part in enumerate(three_parts(y_s[n])):
            parts[BLOCK * (3 + i) : BLOCK * (4 + i), lanes * n : lanes * (n + 1)] = part
    upper = (row_id <= col_id).astype(bf16)
    before = (row_id > col_id).astype(bf16)
    ddecay = mm(jnp.concatenate([upper] * 3 + [before] * 3, axis=1), parts[...])
    bias = jnp.zeros((1, lanes), f32)
    for n in range(blocks):
        pre = pre_s[n]
        e = jnp.exp(-jnp.abs(pre))
        slope = jnp.where(pre >= 0.0, e, 1.0) / (1.0 + e)
        gate = (
            (ddecay[:, lanes * n : lanes * (n + 1)] + e_s[n]) * slope * (1.0 / SMOOTHING)
        ).astype(bf16)
        bias = bias + jnp.sum(gate.astype(f32), axis=0, keepdims=True)
        for p in range(PACK):
            gate_s[rows * n : rows * (n + 1), lanes * p : lanes * (p + 1)] = gate[
                rows * p : rows * (p + 1)
            ]
    gates = gate_s[...]
    lowg = mm(gates, wbig[...], 1, 1)
    goes_ref[:, 4 * BLOCK : 4 * BLOCK + rows] = lowg.reshape(blocks, rows, lanes).astype(bf16)
    cross = mm(low, gates, 0, 0)
    up = cross[:RANK, :lanes]
    for p in range(1, PACK):
        up = up + cross[RANK * p : RANK * (p + 1), lanes * p : lanes * (p + 1)]
    share = RANK // blocks
    for i, part in enumerate(two_parts(up)):
        at = 4 * BLOCK + rows + i * share
        for n in range(blocks):
            goes_ref[n, at : at + share] = part[share * n : share * (n + 1)]
    for i, part in enumerate(two_parts(bias)):
        bias_ref[i : i + 1] = part


def prepare_kernel(head_ref, adj_ref, wide_ref, off_ref, ex_ref, going_ref, wu_ref, offs_ref, column_ref):
    seqs, local_len, _ = adj_ref.shape
    lanes = ADDRESS_WIDTH
    pieces = PAYLOAD_WIDTH // lanes
    for b in range(seqs):
        for h in range(HEADS):
            for i in range(pieces):
                going_ref[b * HEADS + h, local_len * i : local_len * (i + 1)] = adj_ref[
                    b, :, lanes * (h * pieces + i) : lanes * (h * pieces + i + 1)
                ]
    going_ref[:, pieces * local_len :] = jnp.zeros(
        (going_ref.shape[0], going_ref.shape[1] - pieces * local_len, lanes), bf16
    )
    at = pl.multiple_of(head_ref[0] * lanes, lanes)
    wu_ref[...] = wide_ref[:, pl.ds(at, lanes)]
    offs_ref[...] = off_ref[:, pl.ds(at, lanes)]
    blocks = column_ref.shape[1]
    row_id = lax.broadcasted_iota(jnp.int32, (BLOCK, BLOCK), 0)
    col_id = lax.broadcasted_iota(jnp.int32, (BLOCK, BLOCK), 1)
    place = lax.broadcasted_iota(jnp.int32, (BLOCK, blocks), 1)
    columns = jnp.zeros((BLOCK, blocks), f32)
    for n in range(blocks):
        row = ex_ref[:, BLOCK * n : BLOCK * (n + 1)]
        column = jnp.sum(jnp.where(row_id == col_id, row, 0.0), axis=1, keepdims=True)
        columns = jnp.where(place == n, column, columns)
    column_ref[...] = columns


def prepare(head, adj, wide, off, ex):
    seqs, local_len, _ = adj.shape
    rows = PAYLOAD_WIDTH // ADDRESS_WIDTH * local_len + BLOCK // PACK
    everything = pl.BlockSpec(memory_space=pltpu.VMEM)
    return pl.pallas_call(
        prepare_kernel,
        out_shape=(
            jax.ShapeDtypeStruct((seqs * HEADS, rows, ADDRESS_WIDTH), bf16),
            jax.ShapeDtypeStruct((RANK, ADDRESS_WIDTH), bf16),
            jax.ShapeDtypeStruct((1, ADDRESS_WIDTH), f32),
            jax.ShapeDtypeStruct((BLOCK, ex.shape[1] // BLOCK), f32),
        ),
        in_specs=[pl.BlockSpec(memory_space=pltpu.SMEM)] + [everything] * 4,
        name="prepare",
    )(head.astype(jnp.int32)[None], adj, wide, off, ex)


def mixer(came, wu, off, ex, q, k, v):
    blocks = q.shape[0]
    A, V = ADDRESS_WIDTH, PAYLOAD_WIDTH
    rows = BLOCK // PACK
    vmem = lambda shape, dt: pltpu.VMEM(shape, dt)
    return pl.pallas_call(
        mixer_kernel,
        out_shape=(
            jax.ShapeDtypeStruct((blocks, 4 * BLOCK + rows + 2 * RANK // blocks, A), bf16),
            jax.ShapeDtypeStruct((2, A), bf16),
        ),
        scratch_shapes=[
            vmem((A, PACK * A), bf16),
            vmem((6 * BLOCK, blocks * A), bf16),
            vmem((blocks, BLOCK, A), f32),
            vmem((blocks, BLOCK, A), f32),
            vmem((blocks, BLOCK, A), bf16),
            vmem((blocks, BLOCK, A), bf16),
            vmem((blocks, V, A), f32),
            vmem((blocks, BLOCK, BLOCK), bf16),
            vmem((blocks, BLOCK, A), f32),
            vmem((blocks, BLOCK, A), f32),
            vmem((blocks, BLOCK, A), f32),
            vmem((blocks, BLOCK, A), f32),
            vmem((blocks, 1, A), f32),
            vmem((blocks * rows, PACK * A), bf16),
        ],
        name="mixer",
    )(came, wu, off, ex, q, k, v)


def exchanged(tensor, axis):
    return lax.all_to_all(tensor, axis, split_axis=0, concat_axis=0, tiled=True)


def everyones(tensor, axis):
    return exchanged(jnp.broadcast_to(tensor, (lax.axis_size(axis), *tensor.shape)), axis)


def in_rows(tensor, lanes=128):
    flat = tensor.reshape(*tensor.shape[:-2], -1)
    pad = -flat.shape[-1] % lanes
    flat = jnp.pad(flat, [(0, 0)] * (flat.ndim - 1) + [(0, pad)])
    return flat.reshape(*flat.shape[:-1], -1, lanes)


def on_device(
    standardized_block_source,
    forgetting_narrowing_matrix,
    forgetting_widening_matrix,
    forgetting_offset_vector,
    probe_vectors,
    address_vectors,
    payload_vectors,
    extra_channel_forgetting,
    blender_result_adjoint,
):
    seqs, local_len, width = standardized_block_source.shape
    tokens = seqs * local_len
    length = probe_vectors.shape[1]
    blocks = length // BLOCK
    sp = lax.axis_size("sp")
    dp = lax.axis_size("dp")
    part = forgetting_narrowing_matrix.shape[0]
    A, V, R = ADDRESS_WIDTH, PAYLOAD_WIDTH, RANK
    rows = BLOCK // PACK
    contract = (((0,), (0,)), ((), ()))
    flat_input = standardized_block_source.reshape(tokens, width)

    down_rows = everyones(in_rows(forgetting_narrowing_matrix), "dp")
    down = down_rows.reshape(dp, -1)[:, : part * R].reshape(width, R)
    going, columns, offsets, extra = prepare(
        lax.axis_index("sp") % HEADS,
        blender_result_adjoint,
        forgetting_widening_matrix,
        forgetting_offset_vector[None],
        extra_channel_forgetting,
    )
    low = jnp.dot(flat_input, down, preferred_element_type=f32).astype(bf16)
    low = low.reshape(seqs, PACK, rows, R).transpose(0, 2, 1, 3).reshape(seqs, 1, rows, PACK * R)
    low = jnp.broadcast_to(low, (seqs, HEADS, rows, PACK * R)).reshape(sp, rows, A)
    going = lax.dynamic_update_slice(going, low, (0, 2 * BLOCK, 0))
    came = exchanged(going, "sp")
    goes, bias = mixer(
        came,
        columns,
        offsets,
        extra,
        probe_vectors.reshape(blocks, BLOCK, A),
        address_vectors.reshape(blocks, BLOCK, A),
        payload_vectors.reshape(blocks, BLOCK, V),
    )

    share = R // sp
    returned = exchanged(goes, "sp")
    first = returned[:, 4 * BLOCK :].astype(f32)
    low_grad = jnp.sum(first[:, :rows].reshape(seqs, HEADS, rows, A), axis=1).astype(bf16)
    low_grad = low_grad.reshape(seqs, rows, PACK, R).transpose(0, 2, 1, 3).reshape(tokens, R)
    up = first[:, rows : rows + share] + first[:, rows + share : rows + 2 * share]
    up = jnp.sum(up.reshape(seqs, HEADS * share, A), axis=0)

    def to_tokens(start, pieces):
        block = returned[:, start * BLOCK : (start + pieces) * BLOCK]
        block = block.reshape(seqs, HEADS, pieces, local_len, A)
        return block.transpose(0, 3, 1, 2, 4).reshape(seqs, local_len, HEADS * pieces * A)

    grad_input = jnp.dot(low_grad, down.T, preferred_element_type=f32).astype(bf16)
    whole = lax.dot_general(flat_input, low_grad, contract, preferred_element_type=f32)
    whole = in_rows(whole.astype(bf16).reshape(dp, part, R))
    n_whole = whole.shape[1]
    own = jnp.concatenate([up.astype(bf16), bias], axis=0)
    second = exchanged(
        jnp.concatenate([whole, jnp.broadcast_to(own, (dp, *own.shape))], axis=1), "dp"
    )
    second = jnp.sum(second.astype(f32), axis=0)
    second = jnp.concatenate(
        [second[:-2].astype(bf16), *two_parts(second[-2:-1] + second[-1:])], axis=0
    )
    third = everyones(second, "sp").astype(f32)
    down_grad = jnp.sum(third[:, :n_whole], axis=0).reshape(-1)[: part * R].reshape(part, R)
    up_grad = (
        third[:, n_whole:-2]
        .reshape(sp, HEADS, share, A)
        .transpose(0, 2, 1, 3)
        .reshape(R, HEADS * A)
    )
    bias_grad = jnp.sum((third[:, -2] + third[:, -1]).reshape(seqs, HEADS * A), axis=0)
    return (
        to_tokens(0, 1),
        to_tokens(1, 1),
        to_tokens(2, 2),
        grad_input.reshape(seqs, local_len, width),
        down_grad,
        up_grad,
        bias_grad,
    )


def solution(mesh):
    placed = (
        P("dp", "sp", None),
        P("dp", None),
        P(),
        P(),
        P(("dp", "sp"), None, None),
        P(("dp", "sp"), None, None),
        P(("dp", "sp"), None, None),
        P(("dp", "sp"), None),
        P("dp", "sp", None),
    )
    return jax.shard_map(
        on_device,
        mesh=mesh,
        in_specs=placed,
        out_specs=(
            P("dp", "sp", None),
            P("dp", "sp", None),
            P("dp", "sp", None),
            P("dp", "sp", None),
            P("dp", None),
            P(),
            P(),
        ),
        check_vma=False,
    )
```

```python
import jax
import jax.numpy as jnp
from jax import lax
from jax.experimental import pallas as pl
from jax.experimental.pallas import tpu as pltpu
from jax.sharding import PartitionSpec as P

HEADS = 8
ADDRESS_WIDTH = 128
PAYLOAD_WIDTH = 256
RANK = 32
BLOCK = 64
SMOOTHING = 16.0
SPAN_LIMIT = 80.0
PACK = 4
GROUP = 4
UNROLL = 4
f32 = jnp.float32
bf16 = jnp.bfloat16


def mm(a, b, ca=1, cb=0):
    return lax.dot_general(a, b, (((ca,), (cb,)), ((), ())), preferred_element_type=f32)


def two_parts(a):
    hi = a.astype(bf16)
    return hi, (a - hi.astype(f32)).astype(bf16)


def three_parts(a):
    hi = a.astype(bf16)
    return hi, *two_parts(a - hi.astype(f32))


def mixer_kernel(
    came_hbm, wu_ref, off_ref, ex_ref, q_hbm, k_hbm, v_hbm,
    goes_hbm, bias_ref,
    low_s, do_ref, q_ref, k_ref, v_ref, goes_ref, wbig, parts, b_s, pre_s, qp_s, kf_s, st_s,
    pt_s, dqi_s, dki_s, x_s, y_s, e_s, gate_s, sems,
):
    blocks = q_ref.shape[0]
    rows = BLOCK // PACK
    lanes = ADDRESS_WIDTH
    scale = ADDRESS_WIDTH ** (-0.5)
    middle = BLOCK // 2
    group = GROUP * BLOCK
    halves = PAYLOAD_WIDTH // lanes

    copies = [
        pltpu.make_async_copy(came_hbm.at[:, halves * BLOCK :], low_s, sems.at[0]),
        pltpu.make_async_copy(q_hbm, q_ref, sems.at[1]),
        pltpu.make_async_copy(k_hbm, k_ref, sems.at[2]),
        pltpu.make_async_copy(came_hbm.at[:, : halves * BLOCK], do_ref, sems.at[3]),
        pltpu.make_async_copy(v_hbm, v_ref, sems.at[4]),
    ]
    for copy in copies:
        copy.start()

    def do_rows(at, count):
        both = do_ref[pl.ds(at, count)]
        return jnp.concatenate(
            [
                both[:, BLOCK * i : BLOCK * (i + 1)].reshape(count * BLOCK, lanes)
                for i in range(halves)
            ],
            axis=1,
        )

    row_id = lax.broadcasted_iota(jnp.int32, (BLOCK, BLOCK), 0)
    col_id = lax.broadcasted_iota(jnp.int32, (BLOCK, BLOCK), 1)

    wbig[...] = jnp.zeros(wbig.shape, bf16)
    for p in range(PACK):
        wbig[RANK * p : RANK * (p + 1), lanes * p : lanes * (p + 1)] = wu_ref[...]
    copies[0].wait()
    low = low_s[...].reshape(blocks * rows, lanes)
    raw = mm(low, wbig[...])
    offs = off_ref[...]
    for n in range(blocks):
        pre = (
            jnp.concatenate(
                [
                    raw[rows * n : rows * (n + 1), lanes * p : lanes * (p + 1)]
                    for p in range(PACK)
                ],
                axis=0,
            )
            + offs
        )
        pre_s[n] = pre
        decay = (jnp.minimum(pre, 0.0) - jnp.log1p(jnp.exp(-jnp.abs(pre)))) * (
            1.0 / SMOOTHING
        ) + ex_ref[:, n : n + 1]
        for i, part in enumerate(three_parts(decay)):
            parts[BLOCK * i : BLOCK * (i + 1), lanes * n : lanes * (n + 1)] = part
    lower = (row_id >= col_id).astype(bf16)
    sums = mm(jnp.concatenate([lower] * 3, axis=1), parts[: 3 * BLOCK])
    span = jnp.zeros((1, lanes), f32)
    for n in range(blocks):
        b = sums[:, lanes * n : lanes * (n + 1)]
        b_s[n] = b
        centre = b[middle : middle + 1]
        span = jnp.maximum(span, jnp.maximum(b[:1] - centre, centre - b[BLOCK - 1 :]))
    narrow = jnp.max(span) < SPAN_LIMIT
    for copy in copies[1:]:
        copy.wait()

    @pl.when(narrow)
    def _():
        big_row = lax.broadcasted_iota(jnp.int32, (group, group), 0)
        big_col = lax.broadcasted_iota(jnp.int32, (group, group), 1)
        same = big_row // BLOCK == big_col // BLOCK
        causal = same & (big_row >= big_col)
        mirrored = same & (big_row <= big_col)

        def within(g, carry):
            at = g * GROUP
            b = b_s[pl.ds(at, GROUP)]
            centre = b[:, middle : middle + 1]
            lift = jnp.exp(b - centre).reshape(group, lanes)
            drop = jnp.exp(centre - b).reshape(group, lanes)
            q = q_ref[pl.ds(at, GROUP)].astype(f32).reshape(group, lanes)
            k = k_ref[pl.ds(at, GROUP)].astype(f32).reshape(group, lanes)
            qc = (q * scale * lift).astype(bf16)
            kc = (k * drop).astype(bf16)
            do = do_rows(at, GROUP)
            v = v_ref[pl.ds(at, GROUP)].reshape(group, PAYLOAD_WIDTH)
            pt_s[g] = jnp.where(mirrored, mm(kc, qc, 1, 1), 0.0).astype(bf16)
            dp = jnp.where(causal, mm(do, v, 1, 1), 0.0).astype(bf16)
            dq = mm(dp, kc)
            dk = mm(dp, qc, 0, 0)
            shape = (GROUP, BLOCK, lanes)
            x_s[pl.ds(at, GROUP)] = (dq * qc.astype(f32) - dk * kc.astype(f32)).reshape(shape)
            dqi_s[pl.ds(at, GROUP)] = (dq * lift).reshape(shape)
            dki_s[pl.ds(at, GROUP)] = (dk * drop).reshape(shape)
            return carry

        lax.fori_loop(0, blocks // GROUP, within, 0, unroll=UNROLL)

    @pl.when(jnp.logical_not(narrow))
    def _():
        pt_s[...] = jnp.zeros(pt_s.shape, bf16)
        for m in range(GROUP):
            def within(g, carry, m=m):
                n = g * GROUP + m
                b = b_s[n]
                q = q_ref[n].astype(f32) * scale
                dp = mm(do_rows(n, 1), v_ref[n], 1, 1)
                at = lax.broadcasted_iota(jnp.int32, (BLOCK, 1), 0)
                dqi_s[n] = jnp.zeros((BLOCK, lanes), f32)
                x_s[n] = jnp.zeros((BLOCK, lanes), f32)

                def one(s, scores):
                    here = at == s
                    b_row = jnp.sum(jnp.where(here, b, 0.0), axis=0, keepdims=True)
                    k_row = jnp.sum(
                        jnp.where(here, k_ref[n].astype(f32), 0.0), axis=0, keepdims=True
                    )
                    decay = jnp.where(at >= s, jnp.exp(jnp.minimum(b - b_row, 0.0)), 0.0)
                    dp_col = jnp.sum(jnp.where(col_id == s, dp, 0.0), axis=1, keepdims=True)
                    qd = q * decay
                    column = jnp.sum(qd * k_row, axis=1, keepdims=True)
                    dq = dp_col * decay * k_row
                    dk_row = jnp.sum(dp_col * qd, axis=0, keepdims=True)
                    dqi_s[n] = dqi_s[n] + dq
                    dki_s[n] = jnp.where(here, dk_row, dki_s[n])
                    x_s[n] = x_s[n] + q * dq - jnp.where(here, dk_row * k_row, 0.0)
                    return scores + jnp.where(col_id == s, column, 0.0)

                scores = lax.fori_loop(0, BLOCK, one, jnp.zeros((BLOCK, BLOCK), f32))
                pt_s[g, BLOCK * m : BLOCK * (m + 1), BLOCK * m : BLOCK * (m + 1)] = (
                    scores.T.astype(bf16)
                )
                return carry

            lax.fori_loop(0, blocks // GROUP, within, 0)

    def spread(tensor):
        zero = jnp.zeros((BLOCK, lanes), tensor.dtype)
        return jnp.concatenate(
            [
                jnp.concatenate(
                    [tensor[m] if m == i else zero for i in range(GROUP)], axis=0
                )
                for m in range(GROUP)
            ],
            axis=1,
        )

    def forward(g, state):
        at = g * GROUP
        b = b_s[pl.ds(at, GROUP)]
        last = b[:, BLOCK - 1 :]
        grow = jnp.exp(b)
        fade = jnp.exp(last)
        qp = (q_ref[pl.ds(at, GROUP)].astype(f32) * scale * grow).astype(bf16)
        kf = (k_ref[pl.ds(at, GROUP)].astype(f32) * jnp.exp(last - b)).astype(bf16)
        qp_s[pl.ds(at, GROUP)] = qp
        kf_s[pl.ds(at, GROUP)] = kf
        v = v_ref[pl.ds(at, GROUP)].reshape(group, PAYLOAD_WIDTH)
        added = mm(v, spread(kf), 0, 0)
        do = do_rows(at, GROUP)
        for m in range(GROUP):
            n = at + m
            st_s[n] = state
            dq = mm(do[BLOCK * m : BLOCK * (m + 1)], state.astype(bf16))
            x_s[n] = x_s[n] + qp[m].astype(f32) * dq
            goes_ref[n, :BLOCK] = ((dqi_s[n] + dq * grow[m]) * scale).astype(bf16)
            state = state * fade[m] + added[:, lanes * m : lanes * (m + 1)]
        return state

    zero = jnp.zeros((PAYLOAD_WIDTH, lanes), f32)
    lax.fori_loop(0, blocks // GROUP, forward, zero, unroll=UNROLL)
    out_q = pltpu.make_async_copy(
        goes_ref.at[:, :BLOCK], goes_hbm.at[:, :BLOCK], sems.at[5]
    )
    out_q.start()

    def backward(i, dstate):
        g = blocks // GROUP - 1 - i
        at = g * GROUP
        b = b_s[pl.ds(at, GROUP)]
        last = b[:, BLOCK - 1 :]
        drop = jnp.exp(last - b)
        fade = jnp.exp(last)
        do = do_rows(at, GROUP)
        added = mm(do, spread(qp_s[pl.ds(at, GROUP)]), 0, 0)
        dv_own = mm(pt_s[g], do)
        for m in reversed(range(GROUP)):
            n = at + m
            ds = dstate.astype(bf16)
            kf = kf_s[n]
            dk = mm(v_ref[n], ds)
            goes_ref[n, BLOCK : 2 * BLOCK] = (dki_s[n] + dk * drop[m]).astype(bf16)
            dv = (dv_own[BLOCK * m : BLOCK * (m + 1)] + mm(kf, ds, 1, 1)).astype(bf16)
            for i in range(halves):
                goes_ref[n, BLOCK * (2 + i) : BLOCK * (3 + i)] = dv[
                    :, lanes * i : lanes * (i + 1)
                ]
            y_s[n] = kf.astype(f32) * dk
            e_s[n] = fade[m] * jnp.sum(st_s[n] * dstate, axis=0, keepdims=True)
            dstate = dstate * fade[m] + added[:, lanes * m : lanes * (m + 1)]
        return dstate

    lax.fori_loop(0, blocks // GROUP, backward, zero, unroll=UNROLL)
    out_kv = pltpu.make_async_copy(
        goes_ref.at[:, BLOCK : 4 * BLOCK], goes_hbm.at[:, BLOCK : 4 * BLOCK], sems.at[6]
    )
    out_kv.start()

    for n in range(blocks):
        for i, part in enumerate(three_parts(x_s[n])):
            parts[BLOCK * i : BLOCK * (i + 1), lanes * n : lanes * (n + 1)] = part
        for i, part in enumerate(three_parts(y_s[n])):
            parts[BLOCK * (3 + i) : BLOCK * (4 + i), lanes * n : lanes * (n + 1)] = part
    upper = (row_id <= col_id).astype(bf16)
    before = (row_id > col_id).astype(bf16)
    ddecay = mm(jnp.concatenate([upper] * 3 + [before] * 3, axis=1), parts[...])
    bias = jnp.zeros((1, lanes), f32)
    for n in range(blocks):
        pre = pre_s[n]
        e = jnp.exp(-jnp.abs(pre))
        slope = jnp.where(pre >= 0.0, e, 1.0) / (1.0 + e)
        gate = (
            (ddecay[:, lanes * n : lanes * (n + 1)] + e_s[n]) * slope * (1.0 / SMOOTHING)
        ).astype(bf16)
        bias = bias + jnp.sum(gate.astype(f32), axis=0, keepdims=True)
        for p in range(PACK):
            gate_s[rows * n : rows * (n + 1), lanes * p : lanes * (p + 1)] = gate[
                rows * p : rows * (p + 1)
            ]
    gates = gate_s[...]
    lowg = mm(gates, wbig[...], 1, 1)
    first = 4 * BLOCK
    goes_ref[:, first : first + rows] = lowg.reshape(blocks, rows, lanes).astype(bf16)
    cross = mm(low, gates, 0, 0)
    up = cross[:RANK, :lanes]
    for p in range(1, PACK):
        up = up + cross[RANK * p : RANK * (p + 1), lanes * p : lanes * (p + 1)]
    share = RANK // blocks
    for i, part in enumerate(two_parts(up)):
        at = first + rows + i * share
        for n in range(blocks):
            goes_ref[n, at : at + share] = part[share * n : share * (n + 1)]
    for i, part in enumerate(two_parts(bias)):
        bias_ref[i : i + 1] = part
    out_rest = pltpu.make_async_copy(
        goes_ref.at[:, first:], goes_hbm.at[:, first:], sems.at[7]
    )
    out_rest.start()
    out_q.wait()
    out_kv.wait()
    out_rest.wait()


def prepare_kernel(head_ref, adj_ref, wide_ref, off_ref, ex_ref, going_ref, wu_ref, offs_ref, column_ref):
    seqs, local_len, _ = adj_ref.shape
    lanes = ADDRESS_WIDTH
    pieces = PAYLOAD_WIDTH // lanes
    for b in range(seqs):
        for h in range(HEADS):
            for i in range(pieces):
                going_ref[b * HEADS + h, local_len * i : local_len * (i + 1)] = adj_ref[
                    b, :, lanes * (h * pieces + i) : lanes * (h * pieces + i + 1)
                ]
    going_ref[:, pieces * local_len :] = jnp.zeros(
        (going_ref.shape[0], going_ref.shape[1] - pieces * local_len, lanes), bf16
    )
    at = pl.multiple_of(head_ref[0] * lanes, lanes)
    wu_ref[...] = wide_ref[:, pl.ds(at, lanes)]
    offs_ref[...] = off_ref[:, pl.ds(at, lanes)]
    blocks = column_ref.shape[1]
    row_id = lax.broadcasted_iota(jnp.int32, (BLOCK, BLOCK), 0)
    col_id = lax.broadcasted_iota(jnp.int32, (BLOCK, BLOCK), 1)
    place = lax.broadcasted_iota(jnp.int32, (BLOCK, blocks), 1)
    columns = jnp.zeros((BLOCK, blocks), f32)
    for n in range(blocks):
        row = ex_ref[:, BLOCK * n : BLOCK * (n + 1)]
        column = jnp.sum(jnp.where(row_id == col_id, row, 0.0), axis=1, keepdims=True)
        columns = jnp.where(place == n, column, columns)
    column_ref[...] = columns


def prepare(head, adj, wide, off, ex):
    seqs, local_len, _ = adj.shape
    rows = PAYLOAD_WIDTH // ADDRESS_WIDTH * local_len + BLOCK // PACK
    everything = pl.BlockSpec(memory_space=pltpu.VMEM)
    return pl.pallas_call(
        prepare_kernel,
        out_shape=(
            jax.ShapeDtypeStruct((seqs * HEADS, rows, ADDRESS_WIDTH), bf16),
            jax.ShapeDtypeStruct((RANK, ADDRESS_WIDTH), bf16),
            jax.ShapeDtypeStruct((1, ADDRESS_WIDTH), f32),
            jax.ShapeDtypeStruct((BLOCK, ex.shape[1] // BLOCK), f32),
        ),
        in_specs=[pl.BlockSpec(memory_space=pltpu.SMEM)] + [everything] * 4,
        name="prepare",
    )(head.astype(jnp.int32)[None], adj, wide, off, ex)


def mixer(came, wu, off, ex, q, k, v):
    blocks = q.shape[0]
    A, V = ADDRESS_WIDTH, PAYLOAD_WIDTH
    rows = BLOCK // PACK
    height = 4 * BLOCK + rows + 2 * RANK // blocks
    vmem = pltpu.VMEM
    anywhere = pl.BlockSpec(memory_space=pl.ANY)
    inside = pl.BlockSpec(memory_space=pltpu.VMEM)
    return pl.pallas_call(
        mixer_kernel,
        out_shape=(
            jax.ShapeDtypeStruct((blocks, height, A), bf16),
            jax.ShapeDtypeStruct((2, A), bf16),
        ),
        in_specs=[anywhere, inside, inside, inside, anywhere, anywhere, anywhere],
        out_specs=[anywhere, inside],
        scratch_shapes=[
            vmem((blocks, rows, A), bf16),
            vmem((blocks, V // A * BLOCK, A), bf16),
            vmem((blocks, BLOCK, A), bf16),
            vmem((blocks, BLOCK, A), bf16),
            vmem((blocks, BLOCK, V), bf16),
            vmem((blocks, height, A), bf16),
            vmem((A, PACK * A), bf16),
            vmem((6 * BLOCK, blocks * A), bf16),
            vmem((blocks, BLOCK, A), f32),
            vmem((blocks, BLOCK, A), f32),
            vmem((blocks, BLOCK, A), bf16),
            vmem((blocks, BLOCK, A), bf16),
            vmem((blocks, V, A), f32),
            vmem((blocks // GROUP, GROUP * BLOCK, GROUP * BLOCK), bf16),
            vmem((blocks, BLOCK, A), f32),
            vmem((blocks, BLOCK, A), f32),
            vmem((blocks, BLOCK, A), f32),
            vmem((blocks, BLOCK, A), f32),
            vmem((blocks, 1, A), f32),
            vmem((blocks * rows, PACK * A), bf16),
            pltpu.SemaphoreType.DMA((8,)),
        ],
        name="mixer",
    )(came, wu, off, ex, q, k, v)


def exchanged(tensor, axis):
    return lax.all_to_all(tensor, axis, split_axis=0, concat_axis=0, tiled=True)


def everyones(tensor, axis):
    return exchanged(jnp.broadcast_to(tensor, (lax.axis_size(axis), *tensor.shape)), axis)


def in_rows(tensor, lanes=128):
    flat = tensor.reshape(*tensor.shape[:-2], -1)
    pad = -flat.shape[-1] % lanes
    flat = jnp.pad(flat, [(0, 0)] * (flat.ndim - 1) + [(0, pad)])
    return flat.reshape(*flat.shape[:-1], -1, lanes)


def on_device(
    standardized_block_source,
    forgetting_narrowing_matrix,
    forgetting_widening_matrix,
    forgetting_offset_vector,
    probe_vectors,
    address_vectors,
    payload_vectors,
    extra_channel_forgetting,
    blender_result_adjoint,
):
    seqs, local_len, width = standardized_block_source.shape
    tokens = seqs * local_len
    length = probe_vectors.shape[1]
    blocks = length // BLOCK
    sp = lax.axis_size("sp")
    dp = lax.axis_size("dp")
    part = forgetting_narrowing_matrix.shape[0]
    A, V, R = ADDRESS_WIDTH, PAYLOAD_WIDTH, RANK
    rows = BLOCK // PACK
    contract = (((0,), (0,)), ((), ()))
    flat_input = standardized_block_source.reshape(tokens, width)

    down_rows = everyones(in_rows(forgetting_narrowing_matrix), "dp")
    down = down_rows.reshape(dp, -1)[:, : part * R].reshape(width, R)
    going, columns, offsets, extra = prepare(
        lax.axis_index("sp") % HEADS,
        blender_result_adjoint,
        forgetting_widening_matrix,
        forgetting_offset_vector[None],
        extra_channel_forgetting,
    )
    low = jnp.dot(flat_input, down, preferred_element_type=f32).astype(bf16)
    low = low.reshape(seqs, PACK, rows, R).transpose(0, 2, 1, 3).reshape(seqs, 1, rows, PACK * R)
    low = jnp.broadcast_to(low, (seqs, HEADS, rows, PACK * R)).reshape(sp, rows, A)
    going = lax.dynamic_update_slice(going, low, (0, 2 * BLOCK, 0))
    came = exchanged(going, "sp")
    goes, bias = mixer(
        came,
        columns,
        offsets,
        extra,
        probe_vectors.reshape(blocks, BLOCK, A),
        address_vectors.reshape(blocks, BLOCK, A),
        payload_vectors.reshape(blocks, BLOCK, V),
    )

    share = R // sp
    returned = exchanged(goes, "sp")
    first = returned[:, 4 * BLOCK :].astype(f32)
    low_grad = jnp.sum(first[:, :rows].reshape(seqs, HEADS, rows, A), axis=1).astype(bf16)
    low_grad = low_grad.reshape(seqs, rows, PACK, R).transpose(0, 2, 1, 3).reshape(tokens, R)
    up = first[:, rows : rows + share] + first[:, rows + share : rows + 2 * share]
    up = jnp.sum(up.reshape(seqs, HEADS * share, A), axis=0)

    def to_tokens(start, pieces):
        block = returned[:, start * BLOCK : (start + pieces) * BLOCK]
        block = block.reshape(seqs, HEADS, pieces, local_len, A)
        return block.transpose(0, 3, 1, 2, 4).reshape(seqs, local_len, HEADS * pieces * A)

    grad_input = jnp.dot(low_grad, down.T, preferred_element_type=f32).astype(bf16)
    whole = lax.dot_general(flat_input, low_grad, contract, preferred_element_type=f32)
    whole = in_rows(whole.astype(bf16).reshape(dp, part, R))
    n_whole = whole.shape[1]
    own = jnp.concatenate([up.astype(bf16), bias], axis=0)
    second = exchanged(
        jnp.concatenate([whole, jnp.broadcast_to(own, (dp, *own.shape))], axis=1), "dp"
    )
    second = jnp.sum(second.astype(f32), axis=0)
    second = jnp.concatenate(
        [second[:-2].astype(bf16), *two_parts(second[-2:-1] + second[-1:])], axis=0
    )
    third = everyones(second, "sp").astype(f32)
    down_grad = jnp.sum(third[:, :n_whole], axis=0).reshape(-1)[: part * R].reshape(part, R)
    up_grad = (
        third[:, n_whole:-2]
        .reshape(sp, HEADS, share, A)
        .transpose(0, 2, 1, 3)
        .reshape(R, HEADS * A)
    )
    bias_grad = jnp.sum((third[:, -2] + third[:, -1]).reshape(seqs, HEADS * A), axis=0)
    return (
        to_tokens(0, 1),
        to_tokens(1, 1),
        to_tokens(2, 2),
        grad_input.reshape(seqs, local_len, width),
        down_grad,
        up_grad,
        bias_grad,
    )


def solution(mesh):
    placed = (
        P("dp", "sp", None),
        P("dp", None),
        P(),
        P(),
        P(("dp", "sp"), None, None),
        P(("dp", "sp"), None, None),
        P(("dp", "sp"), None, None),
        P(("dp", "sp"), None),
        P("dp", "sp", None),
    )
    return jax.shard_map(
        on_device,
        mesh=mesh,
        in_specs=placed,
        out_specs=(
            P("dp", "sp", None),
            P("dp", "sp", None),
            P("dp", "sp", None),
            P("dp", "sp", None),
            P("dp", None),
            P(),
            P(),
        ),
        check_vma=False,
    )
```

```python
import jax
import jax.numpy as jnp
from jax import lax
from jax.experimental import pallas as pl
from jax.experimental.pallas import tpu as pltpu
from jax.sharding import PartitionSpec as P

HEADS = 8
ADDRESS_WIDTH = 128
PAYLOAD_WIDTH = 256
RANK = 32
BLOCK = 64
SMOOTHING = 16.0
SPAN_LIMIT = 80.0
PACK = 4
GROUP = 4
NEAR = 4
UNROLL = 4
f32 = jnp.float32
bf16 = jnp.bfloat16


def mm(a, b, ca=1, cb=0):
    return lax.dot_general(a, b, (((ca,), (cb,)), ((), ())), preferred_element_type=f32)


def two_parts(a):
    hi = a.astype(bf16)
    return hi, (a - hi.astype(f32)).astype(bf16)


def three_parts(a):
    hi = a.astype(bf16)
    return hi, *two_parts(a - hi.astype(f32))


def mixer_kernel(
    came_hbm, wu_hbm, off_hbm, ex_hbm, q_hbm, k_hbm, v_hbm,
    goes_hbm, bias_hbm,
    wu_ref, off_ref, ex_ref, bias_ref, low_s, do_ref, q_ref, k_ref, v_ref, goes_ref, wbig, parts, b_s, pre_s, qp_s, kf_s, st_s,
    pt_s, dqi_s, dki_s, x_s, y_s, e_s, gate_s, sems,
):
    blocks = q_ref.shape[0]
    rows = BLOCK // PACK
    lanes = ADDRESS_WIDTH
    scale = ADDRESS_WIDTH ** (-0.5)
    middle = BLOCK // 2
    group = GROUP * BLOCK
    halves = PAYLOAD_WIDTH // lanes

    copies = [
        pltpu.make_async_copy(came_hbm.at[:, halves * BLOCK :], low_s, sems.at[0]),
        pltpu.make_async_copy(wu_hbm, wu_ref, sems.at[8]),
        pltpu.make_async_copy(off_hbm, off_ref, sems.at[9]),
        pltpu.make_async_copy(ex_hbm, ex_ref, sems.at[10]),
        pltpu.make_async_copy(q_hbm, q_ref, sems.at[1]),
        pltpu.make_async_copy(k_hbm, k_ref, sems.at[2]),
        pltpu.make_async_copy(came_hbm.at[:, : halves * BLOCK], do_ref, sems.at[3]),
        pltpu.make_async_copy(v_hbm, v_ref, sems.at[4]),
    ]
    for copy in copies:
        copy.start()

    def do_rows(at, count):
        both = do_ref[pl.ds(at, count)]
        return jnp.concatenate(
            [
                both[:, BLOCK * i : BLOCK * (i + 1)].reshape(count * BLOCK, lanes)
                for i in range(halves)
            ],
            axis=1,
        )

    row_id = lax.broadcasted_iota(jnp.int32, (BLOCK, BLOCK), 0)
    col_id = lax.broadcasted_iota(jnp.int32, (BLOCK, BLOCK), 1)

    wbig[...] = jnp.zeros(wbig.shape, bf16)
    for copy in copies[:4]:
        copy.wait()
    for p in range(PACK):
        wbig[RANK * p : RANK * (p + 1), lanes * p : lanes * (p + 1)] = wu_ref[...]
    low = low_s[...].reshape(blocks * rows, lanes)
    raw = mm(low, wbig[...])
    offs = off_ref[...]
    for n in range(blocks):
        pre = (
            jnp.concatenate(
                [
                    raw[rows * n : rows * (n + 1), lanes * p : lanes * (p + 1)]
                    for p in range(PACK)
                ],
                axis=0,
            )
            + offs
        )
        pre_s[n] = pre
        decay = (jnp.minimum(pre, 0.0) - jnp.log1p(jnp.exp(-jnp.abs(pre)))) * (
            1.0 / SMOOTHING
        ) + ex_ref[:, n : n + 1]
        for i, part in enumerate(three_parts(decay)):
            parts[BLOCK * i : BLOCK * (i + 1), lanes * n : lanes * (n + 1)] = part
    lower = (row_id >= col_id).astype(bf16)
    sums = mm(jnp.concatenate([lower] * 3, axis=1), parts[: 3 * BLOCK])
    span = jnp.zeros((1, lanes), f32)
    for n in range(blocks):
        b = sums[:, lanes * n : lanes * (n + 1)]
        b_s[n] = b
        centre = b[middle : middle + 1]
        span = jnp.maximum(span, jnp.maximum(b[:1] - centre, centre - b[BLOCK - 1 :]))
    narrow = jnp.max(span) < SPAN_LIMIT
    for copy in copies[4:]:
        copy.wait()

    @pl.when(narrow)
    def _():
        big_row = lax.broadcasted_iota(jnp.int32, (group, group), 0)
        big_col = lax.broadcasted_iota(jnp.int32, (group, group), 1)
        same = big_row // BLOCK == big_col // BLOCK
        causal = same & (big_row >= big_col)
        mirrored = same & (big_row <= big_col)

        def within(g, carry):
            at = g * GROUP
            b = b_s[pl.ds(at, GROUP)]
            centre = b[:, middle : middle + 1]
            lift = jnp.exp(b - centre).reshape(group, lanes)
            drop = jnp.exp(centre - b).reshape(group, lanes)
            q = q_ref[pl.ds(at, GROUP)].astype(f32).reshape(group, lanes)
            k = k_ref[pl.ds(at, GROUP)].astype(f32).reshape(group, lanes)
            qc = (q * scale * lift).astype(bf16)
            kc = (k * drop).astype(bf16)
            do = do_rows(at, GROUP)
            v = v_ref[pl.ds(at, GROUP)].reshape(group, PAYLOAD_WIDTH)
            pt_s[g] = jnp.where(mirrored, mm(kc, qc, 1, 1), 0.0).astype(bf16)
            dp = jnp.where(causal, mm(do, v, 1, 1), 0.0).astype(bf16)
            dq = mm(dp, kc)
            dk = mm(dp, qc, 0, 0)
            shape = (GROUP, BLOCK, lanes)
            x_s[pl.ds(at, GROUP)] = (dq * qc.astype(f32) - dk * kc.astype(f32)).reshape(shape)
            dqi_s[pl.ds(at, GROUP)] = (dq * lift).reshape(shape)
            dki_s[pl.ds(at, GROUP)] = (dk * drop).reshape(shape)
            return carry

        lax.fori_loop(0, blocks // GROUP, within, 0, unroll=UNROLL)

    @pl.when(jnp.logical_not(narrow))
    def _():
        pt_s[...] = jnp.zeros(pt_s.shape, bf16)
        for m in range(GROUP):
            def within(g, carry, m=m):
                n = g * GROUP + m
                b = b_s[n]
                q = q_ref[n].astype(f32) * scale
                dp = mm(do_rows(n, 1), v_ref[n], 1, 1)
                at = lax.broadcasted_iota(jnp.int32, (BLOCK, 1), 0)
                dqi_s[n] = jnp.zeros((BLOCK, lanes), f32)
                x_s[n] = jnp.zeros((BLOCK, lanes), f32)

                def one(s, scores):
                    here = at == s
                    b_row = jnp.sum(jnp.where(here, b, 0.0), axis=0, keepdims=True)
                    k_row = jnp.sum(
                        jnp.where(here, k_ref[n].astype(f32), 0.0), axis=0, keepdims=True
                    )
                    decay = jnp.where(at >= s, jnp.exp(jnp.minimum(b - b_row, 0.0)), 0.0)
                    dp_col = jnp.sum(jnp.where(col_id == s, dp, 0.0), axis=1, keepdims=True)
                    qd = q * decay
                    column = jnp.sum(qd * k_row, axis=1, keepdims=True)
                    dq = dp_col * decay * k_row
                    dk_row = jnp.sum(dp_col * qd, axis=0, keepdims=True)
                    dqi_s[n] = dqi_s[n] + dq
                    dki_s[n] = jnp.where(here, dk_row, dki_s[n])
                    x_s[n] = x_s[n] + q * dq - jnp.where(here, dk_row * k_row, 0.0)
                    return scores + jnp.where(col_id == s, column, 0.0)

                scores = lax.fori_loop(0, BLOCK, one, jnp.zeros((BLOCK, BLOCK), f32))
                pt_s[g, BLOCK * m : BLOCK * (m + 1), BLOCK * m : BLOCK * (m + 1)] = (
                    scores.T.astype(bf16)
                )
                return carry

            lax.fori_loop(0, blocks // GROUP, within, 0)

    def spread(tensor):
        zero = jnp.zeros((BLOCK, lanes), tensor.dtype)
        return jnp.concatenate(
            [
                jnp.concatenate(
                    [tensor[m] if m == i else zero for i in range(GROUP)], axis=0
                )
                for m in range(GROUP)
            ],
            axis=1,
        )

    def forward(g, state):
        at = g * GROUP
        b = b_s[pl.ds(at, GROUP)]
        last = b[:, BLOCK - 1 :]
        grow = jnp.exp(b)
        fade = jnp.exp(last)
        qp = (q_ref[pl.ds(at, GROUP)].astype(f32) * scale * grow).astype(bf16)
        kf = (k_ref[pl.ds(at, GROUP)].astype(f32) * jnp.exp(last - b)).astype(bf16)
        qp_s[pl.ds(at, GROUP)] = qp
        kf_s[pl.ds(at, GROUP)] = kf
        v = v_ref[pl.ds(at, GROUP)].reshape(group, PAYLOAD_WIDTH)
        added = mm(v, spread(kf), 0, 0)
        do = do_rows(at, GROUP)
        for m in range(GROUP):
            n = at + m
            st_s[n] = state
            dq = mm(do[BLOCK * m : BLOCK * (m + 1)], state.astype(bf16))
            x_s[n] = x_s[n] + qp[m].astype(f32) * dq
            goes_ref[n, :BLOCK] = ((dqi_s[n] + dq * grow[m]) * scale).astype(bf16)
            state = state * fade[m] + added[:, lanes * m : lanes * (m + 1)]
        return state

    zero = jnp.zeros((PAYLOAD_WIDTH, lanes), f32)
    lax.fori_loop(0, blocks // GROUP, forward, zero, unroll=UNROLL)
    out_q = pltpu.make_async_copy(
        goes_ref.at[:, :BLOCK], goes_hbm.at[:, :BLOCK], sems.at[5]
    )
    out_q.start()

    def backward(i, dstate):
        g = blocks // GROUP - 1 - i
        at = g * GROUP
        b = b_s[pl.ds(at, GROUP)]
        last = b[:, BLOCK - 1 :]
        drop = jnp.exp(last - b)
        fade = jnp.exp(last)
        do = do_rows(at, GROUP)
        added = mm(do, spread(qp_s[pl.ds(at, GROUP)]), 0, 0)
        dv_own = mm(pt_s[g], do)
        for m in reversed(range(GROUP)):
            n = at + m
            ds = dstate.astype(bf16)
            kf = kf_s[n]
            dk = mm(v_ref[n], ds)
            goes_ref[n, BLOCK : 2 * BLOCK] = (dki_s[n] + dk * drop[m]).astype(bf16)
            dv = (dv_own[BLOCK * m : BLOCK * (m + 1)] + mm(kf, ds, 1, 1)).astype(bf16)
            for i in range(halves):
                goes_ref[n, BLOCK * (2 + i) : BLOCK * (3 + i)] = dv[
                    :, lanes * i : lanes * (i + 1)
                ]
            y_s[n] = kf.astype(f32) * dk
            e_s[n] = fade[m] * jnp.sum(st_s[n] * dstate, axis=0, keepdims=True)
            dstate = dstate * fade[m] + added[:, lanes * m : lanes * (m + 1)]
        return dstate

    lax.fori_loop(0, blocks // GROUP, backward, zero, unroll=UNROLL)
    out_kv = pltpu.make_async_copy(
        goes_ref.at[:, BLOCK : 4 * BLOCK], goes_hbm.at[:, BLOCK : 4 * BLOCK], sems.at[6]
    )
    out_kv.start()

    for n in range(blocks):
        for i, part in enumerate(three_parts(x_s[n])):
            parts[BLOCK * i : BLOCK * (i + 1), lanes * n : lanes * (n + 1)] = part
        for i, part in enumerate(three_parts(y_s[n])):
            parts[BLOCK * (3 + i) : BLOCK * (4 + i), lanes * n : lanes * (n + 1)] = part
    upper = (row_id <= col_id).astype(bf16)
    before = (row_id > col_id).astype(bf16)
    ddecay = mm(jnp.concatenate([upper] * 3 + [before] * 3, axis=1), parts[...])
    bias = jnp.zeros((1, lanes), f32)
    for n in range(blocks):
        pre = pre_s[n]
        e = jnp.exp(-jnp.abs(pre))
        slope = jnp.where(pre >= 0.0, e, 1.0) / (1.0 + e)
        gate = (
            (ddecay[:, lanes * n : lanes * (n + 1)] + e_s[n]) * slope * (1.0 / SMOOTHING)
        ).astype(bf16)
        bias = bias + jnp.sum(gate.astype(f32), axis=0, keepdims=True)
        for p in range(PACK):
            gate_s[rows * n : rows * (n + 1), lanes * p : lanes * (p + 1)] = gate[
                rows * p : rows * (p + 1)
            ]
    gates = gate_s[...]
    lowg = mm(gates, wbig[...], 1, 1)
    first = 4 * BLOCK
    goes_ref[:, first : first + rows] = lowg.reshape(blocks, rows, lanes).astype(bf16)
    cross = mm(low, gates, 0, 0)
    up = cross[:RANK, :lanes]
    for p in range(1, PACK):
        up = up + cross[RANK * p : RANK * (p + 1), lanes * p : lanes * (p + 1)]
    share = RANK // blocks
    for i, part in enumerate(two_parts(up)):
        at = first + rows + i * share
        for n in range(blocks):
            goes_ref[n, at : at + share] = part[share * n : share * (n + 1)]
    for i, part in enumerate(two_parts(bias)):
        bias_ref[i : i + 1] = part
    out_rest = pltpu.make_async_copy(
        goes_ref.at[:, first:], goes_hbm.at[:, first:], sems.at[7]
    )
    out_rest.start()
    out_bias = pltpu.make_async_copy(bias_ref, bias_hbm, sems.at[11])
    out_bias.start()
    out_bias.wait()
    out_q.wait()
    out_kv.wait()
    out_rest.wait()


def prepare_kernel(head_ref, adj_ref, wide_ref, off_ref, ex_ref, going_ref, wu_ref, offs_ref, column_ref):
    seqs, local_len, _ = adj_ref.shape
    lanes = ADDRESS_WIDTH
    pieces = PAYLOAD_WIDTH // lanes
    for b in range(seqs):
        for h in range(HEADS):
            for i in range(pieces):
                going_ref[b * HEADS + h, local_len * i : local_len * (i + 1)] = adj_ref[
                    b, :, lanes * (h * pieces + i) : lanes * (h * pieces + i + 1)
                ]
    going_ref[:, pieces * local_len :] = jnp.zeros(
        (going_ref.shape[0], going_ref.shape[1] - pieces * local_len, lanes), bf16
    )
    at = pl.multiple_of(head_ref[0] * lanes, lanes)
    wu_ref[...] = wide_ref[:, pl.ds(at, lanes)]
    offs_ref[...] = off_ref[:, pl.ds(at, lanes)]
    blocks = column_ref.shape[1]
    row_id = lax.broadcasted_iota(jnp.int32, (BLOCK, BLOCK), 0)
    col_id = lax.broadcasted_iota(jnp.int32, (BLOCK, BLOCK), 1)
    place = lax.broadcasted_iota(jnp.int32, (BLOCK, blocks), 1)
    columns = jnp.zeros((BLOCK, blocks), f32)
    for n in range(blocks):
        row = ex_ref[:, BLOCK * n : BLOCK * (n + 1)]
        column = jnp.sum(jnp.where(row_id == col_id, row, 0.0), axis=1, keepdims=True)
        columns = jnp.where(place == n, column, columns)
    column_ref[...] = columns


def prepare(head, adj, wide, off, ex):
    seqs, local_len, _ = adj.shape
    rows = PAYLOAD_WIDTH // ADDRESS_WIDTH * local_len + BLOCK // PACK
    everything = pl.BlockSpec(memory_space=pltpu.VMEM)
    return pl.pallas_call(
        prepare_kernel,
        out_shape=(
            jax.ShapeDtypeStruct((seqs * HEADS, rows, ADDRESS_WIDTH), bf16),
            jax.ShapeDtypeStruct((RANK, ADDRESS_WIDTH), bf16),
            jax.ShapeDtypeStruct((1, ADDRESS_WIDTH), f32),
            jax.ShapeDtypeStruct((BLOCK, ex.shape[1] // BLOCK), f32),
        ),
        in_specs=[pl.BlockSpec(memory_space=pltpu.SMEM)] + [everything] * 4,
        name="prepare",
    )(head.astype(jnp.int32)[None], adj, wide, off, ex)


def mixer(came, wu, off, ex, q, k, v):
    blocks = q.shape[0]
    A, V = ADDRESS_WIDTH, PAYLOAD_WIDTH
    rows = BLOCK // PACK
    height = 4 * BLOCK + rows + 2 * RANK // blocks
    vmem = pltpu.VMEM
    anywhere = pl.BlockSpec(memory_space=pl.ANY)
    return pl.pallas_call(
        mixer_kernel,
        out_shape=(
            jax.ShapeDtypeStruct((blocks, height, A), bf16),
            jax.ShapeDtypeStruct((2, A), bf16),
        ),
        in_specs=[anywhere] * 7,
        out_specs=[anywhere] * 2,
        scratch_shapes=[
            vmem((RANK, A), bf16),
            vmem((1, A), f32),
            vmem((BLOCK, blocks), f32),
            vmem((2, A), bf16),
            vmem((blocks, rows, A), bf16),
            vmem((blocks, V // A * BLOCK, A), bf16),
            vmem((blocks, BLOCK, A), bf16),
            vmem((blocks, BLOCK, A), bf16),
            vmem((blocks, BLOCK, V), bf16),
            vmem((blocks, height, A), bf16),
            vmem((A, PACK * A), bf16),
            vmem((6 * BLOCK, blocks * A), bf16),
            vmem((blocks, BLOCK, A), f32),
            vmem((blocks, BLOCK, A), f32),
            vmem((blocks, BLOCK, A), bf16),
            vmem((blocks, BLOCK, A), bf16),
            vmem((blocks, V, A), f32),
            vmem((blocks // GROUP, GROUP * BLOCK, GROUP * BLOCK), bf16),
            vmem((blocks, BLOCK, A), f32),
            vmem((blocks, BLOCK, A), f32),
            vmem((blocks, BLOCK, A), f32),
            vmem((blocks, BLOCK, A), f32),
            vmem((blocks, 1, A), f32),
            vmem((blocks * rows, PACK * A), bf16),
            pltpu.SemaphoreType.DMA((12,)),
        ],
        name="mixer",
    )(came, wu, off, ex, q, k, v)


def exchanged(tensor, axis, groups=None):
    return lax.all_to_all(
        tensor, axis, split_axis=0, concat_axis=0, tiled=True, axis_index_groups=groups
    )


def everyones(tensor, axis):
    return exchanged(jnp.broadcast_to(tensor, (lax.axis_size(axis), *tensor.shape)), axis)


def in_rows(tensor, lanes=128):
    flat = tensor.reshape(*tensor.shape[:-2], -1)
    pad = -flat.shape[-1] % lanes
    flat = jnp.pad(flat, [(0, 0)] * (flat.ndim - 1) + [(0, pad)])
    return flat.reshape(*flat.shape[:-1], -1, lanes)


def on_device(
    standardized_block_source,
    forgetting_narrowing_matrix,
    forgetting_widening_matrix,
    forgetting_offset_vector,
    probe_vectors,
    address_vectors,
    payload_vectors,
    extra_channel_forgetting,
    blender_result_adjoint,
):
    seqs, local_len, width = standardized_block_source.shape
    tokens = seqs * local_len
    length = probe_vectors.shape[1]
    blocks = length // BLOCK
    sp = lax.axis_size("sp")
    dp = lax.axis_size("dp")
    part = forgetting_narrowing_matrix.shape[0]
    A, V, R = ADDRESS_WIDTH, PAYLOAD_WIDTH, RANK
    rows = BLOCK // PACK
    contract = (((0,), (0,)), ((), ()))
    flat_input = standardized_block_source.reshape(tokens, width)

    down_rows = everyones(in_rows(forgetting_narrowing_matrix), "dp")
    down = down_rows.reshape(dp, -1)[:, : part * R].reshape(width, R)
    going, columns, offsets, extra = prepare(
        lax.axis_index("sp") % HEADS,
        blender_result_adjoint,
        forgetting_widening_matrix,
        forgetting_offset_vector[None],
        extra_channel_forgetting,
    )
    low = jnp.dot(flat_input, down, preferred_element_type=f32).astype(bf16)
    low = low.reshape(seqs, PACK, rows, R).transpose(0, 2, 1, 3).reshape(seqs, 1, rows, PACK * R)
    low = jnp.broadcast_to(low, (seqs, HEADS, rows, PACK * R)).reshape(sp, rows, A)
    going = lax.dynamic_update_slice(going, low, (0, 2 * BLOCK, 0))
    came = exchanged(going, "sp")
    goes, bias = mixer(
        came,
        columns,
        offsets,
        extra,
        probe_vectors.reshape(blocks, BLOCK, A),
        address_vectors.reshape(blocks, BLOCK, A),
        payload_vectors.reshape(blocks, BLOCK, V),
    )

    share = R // sp
    returned = exchanged(goes, "sp")
    first = returned[:, 4 * BLOCK :].astype(f32)
    low_grad = jnp.sum(first[:, :rows].reshape(seqs, HEADS, rows, A), axis=1).astype(bf16)
    low_grad = low_grad.reshape(seqs, rows, PACK, R).transpose(0, 2, 1, 3).reshape(tokens, R)
    up = first[:, rows : rows + share] + first[:, rows + share : rows + 2 * share]
    up = jnp.sum(up.reshape(seqs, HEADS * share, A), axis=0)

    def to_tokens(start, pieces):
        block = returned[:, start * BLOCK : (start + pieces) * BLOCK]
        block = block.reshape(seqs, HEADS, pieces, local_len, A)
        return block.transpose(0, 3, 1, 2, 4).reshape(seqs, local_len, HEADS * pieces * A)

    grad_input = jnp.dot(low_grad, down.T, preferred_element_type=f32).astype(bf16)
    whole = lax.dot_general(flat_input, low_grad, contract, preferred_element_type=f32)
    whole = in_rows(whole.astype(bf16).reshape(dp, part, R))
    n_whole = whole.shape[1]
    own = jnp.concatenate([up.astype(bf16), bias], axis=0)
    near, far = NEAR, dp // NEAR
    near_groups = [[z * near + x for x in range(near)] for z in range(far)]
    far_groups = [[z * near + x for z in range(far)] for x in range(near)]

    def shared(pieces, rest, groups):
        count = len(groups[0])
        payload = jnp.concatenate(
            [pieces.reshape(count, -1, A), jnp.broadcast_to(rest, (count, *rest.shape))], axis=1
        )
        return jnp.sum(exchanged(payload, "dp", groups).astype(f32), axis=0)

    def bias_kept(total):
        return jnp.concatenate(
            [total[:-2].astype(bf16), *two_parts(total[-2:-1] + total[-1:])], axis=0
        )

    whole = whole.reshape(far, near, n_whole, A).transpose(1, 0, 2, 3)
    second = bias_kept(shared(whole, own, near_groups))
    second = bias_kept(
        shared(
            second[: far * n_whole].reshape(far, n_whole, A), second[far * n_whole :], far_groups
        )
    )
    third = everyones(second, "sp").astype(f32)
    down_grad = jnp.sum(third[:, :n_whole], axis=0).reshape(-1)[: part * R].reshape(part, R)
    up_grad = (
        third[:, n_whole:-2]
        .reshape(sp, HEADS, share, A)
        .transpose(0, 2, 1, 3)
        .reshape(R, HEADS * A)
    )
    bias_grad = jnp.sum((third[:, -2] + third[:, -1]).reshape(seqs, HEADS * A), axis=0)
    return (
        to_tokens(0, 1),
        to_tokens(1, 1),
        to_tokens(2, 2),
        grad_input.reshape(seqs, local_len, width),
        down_grad,
        up_grad,
        bias_grad,
    )


def solution(mesh):
    placed = (
        P("dp", "sp", None),
        P("dp", None),
        P(),
        P(),
        P(("dp", "sp"), None, None),
        P(("dp", "sp"), None, None),
        P(("dp", "sp"), None, None),
        P(("dp", "sp"), None),
        P("dp", "sp", None),
    )
    return jax.shard_map(
        on_device,
        mesh=mesh,
        in_specs=placed,
        out_specs=(
            P("dp", "sp", None),
            P("dp", "sp", None),
            P("dp", "sp", None),
            P("dp", "sp", None),
            P("dp", None),
            P(),
            P(),
        ),
        check_vma=False,
    )
```

```python
import jax
import jax.numpy as jnp
from jax import lax
from jax.experimental import pallas as pl
from jax.experimental.pallas import tpu as pltpu
from jax.sharding import PartitionSpec as P

HEADS = 8
ADDRESS_WIDTH = 128
PAYLOAD_WIDTH = 256
RANK = 32
BLOCK = 64
SMOOTHING = 16.0
SPAN_LIMIT = 80.0
PACK = 4
GROUP = 4
NEAR = 4
UNROLL = 4
f32 = jnp.float32
bf16 = jnp.bfloat16


def mm(a, b, ca=1, cb=0):
    return lax.dot_general(a, b, (((ca,), (cb,)), ((), ())), preferred_element_type=f32)


def two_parts(a):
    hi = a.astype(bf16)
    return hi, (a - hi.astype(f32)).astype(bf16)


def three_parts(a):
    hi = a.astype(bf16)
    return hi, *two_parts(a - hi.astype(f32))


def mixer_kernel(
    came_hbm, wu_hbm, off_hbm, ex_hbm, q_hbm, k_hbm, v_hbm,
    goes_hbm, bias_hbm,
    wu_ref, off_ref, ex_ref, bias_ref, low_s, do_ref, q_ref, k_ref, v_ref, goes_ref, wbig, parts, b_s, pre_s, qp_s, kf_s, st_s,
    pt_s, dqi_s, dki_s, x_s, y_s, e_s, gate_s, sems,
):
    blocks = q_ref.shape[0]
    rows = BLOCK // PACK
    lanes = ADDRESS_WIDTH
    scale = ADDRESS_WIDTH ** (-0.5)
    middle = BLOCK // 2
    group = GROUP * BLOCK
    halves = PAYLOAD_WIDTH // lanes

    copies = [
        pltpu.make_async_copy(came_hbm.at[:, halves * BLOCK :], low_s, sems.at[0]),
        pltpu.make_async_copy(wu_hbm, wu_ref, sems.at[8]),
        pltpu.make_async_copy(off_hbm, off_ref, sems.at[9]),
        pltpu.make_async_copy(ex_hbm, ex_ref, sems.at[10]),
        pltpu.make_async_copy(q_hbm, q_ref, sems.at[1]),
        pltpu.make_async_copy(k_hbm, k_ref, sems.at[2]),
        pltpu.make_async_copy(came_hbm.at[:, : halves * BLOCK], do_ref, sems.at[3]),
        pltpu.make_async_copy(v_hbm, v_ref, sems.at[4]),
    ]
    for copy in copies:
        copy.start()

    def do_rows(at, count):
        both = do_ref[pl.ds(at, count)]
        return jnp.concatenate(
            [
                both[:, BLOCK * i : BLOCK * (i + 1)].reshape(count * BLOCK, lanes)
                for i in range(halves)
            ],
            axis=1,
        )

    row_id = lax.broadcasted_iota(jnp.int32, (BLOCK, BLOCK), 0)
    col_id = lax.broadcasted_iota(jnp.int32, (BLOCK, BLOCK), 1)

    wbig[...] = jnp.zeros(wbig.shape, bf16)
    for copy in copies[:4]:
        copy.wait()
    for p in range(PACK):
        wbig[RANK * p : RANK * (p + 1), lanes * p : lanes * (p + 1)] = wu_ref[...]
    low = low_s[...].reshape(blocks * rows, lanes)
    raw = mm(low, wbig[...])
    offs = off_ref[...]
    for n in range(blocks):
        pre = (
            jnp.concatenate(
                [
                    raw[rows * n : rows * (n + 1), lanes * p : lanes * (p + 1)]
                    for p in range(PACK)
                ],
                axis=0,
            )
            + offs
        )
        pre_s[n] = pre
        decay = (jnp.minimum(pre, 0.0) - jnp.log1p(jnp.exp(-jnp.abs(pre)))) * (
            1.0 / SMOOTHING
        ) + ex_ref[:, n : n + 1]
        for i, part in enumerate(three_parts(decay)):
            parts[BLOCK * i : BLOCK * (i + 1), lanes * n : lanes * (n + 1)] = part
    lower = (row_id >= col_id).astype(bf16)
    sums = mm(jnp.concatenate([lower] * 3, axis=1), parts[: 3 * BLOCK])
    span = jnp.zeros((1, lanes), f32)
    for n in range(blocks):
        b = sums[:, lanes * n : lanes * (n + 1)]
        b_s[n] = b
        centre = b[middle : middle + 1]
        span = jnp.maximum(span, jnp.maximum(b[:1] - centre, centre - b[BLOCK - 1 :]))
    narrow = jnp.max(span) < SPAN_LIMIT
    for copy in copies[4:]:
        copy.wait()

    @pl.when(narrow)
    def _():
        big_row = lax.broadcasted_iota(jnp.int32, (group, group), 0)
        big_col = lax.broadcasted_iota(jnp.int32, (group, group), 1)
        same = big_row // BLOCK == big_col // BLOCK
        causal = same & (big_row >= big_col)
        mirrored = same & (big_row <= big_col)

        def within(g, carry):
            at = g * GROUP
            b = b_s[pl.ds(at, GROUP)]
            centre = b[:, middle : middle + 1]
            lift = jnp.exp(b - centre).reshape(group, lanes)
            drop = jnp.exp(centre - b).reshape(group, lanes)
            q = q_ref[pl.ds(at, GROUP)].astype(f32).reshape(group, lanes)
            k = k_ref[pl.ds(at, GROUP)].astype(f32).reshape(group, lanes)
            qc = (q * scale * lift).astype(bf16)
            kc = (k * drop).astype(bf16)
            do = do_rows(at, GROUP)
            v = v_ref[pl.ds(at, GROUP)].reshape(group, PAYLOAD_WIDTH)
            pt_s[g] = jnp.where(mirrored, mm(kc, qc, 1, 1), 0.0).astype(bf16)
            dp = jnp.where(causal, mm(do, v, 1, 1), 0.0).astype(bf16)
            dq = mm(dp, kc)
            dk = mm(dp, qc, 0, 0)
            shape = (GROUP, BLOCK, lanes)
            x_s[pl.ds(at, GROUP)] = (dq * qc.astype(f32) - dk * kc.astype(f32)).reshape(shape)
            dqi_s[pl.ds(at, GROUP)] = (dq * lift).reshape(shape)
            dki_s[pl.ds(at, GROUP)] = (dk * drop).reshape(shape)
            return carry

        lax.fori_loop(0, blocks // GROUP, within, 0, unroll=UNROLL)

    @pl.when(jnp.logical_not(narrow))
    def _():
        pt_s[...] = jnp.zeros(pt_s.shape, bf16)
        for m in range(GROUP):
            def within(g, carry, m=m):
                n = g * GROUP + m
                b = b_s[n]
                q = q_ref[n].astype(f32) * scale
                dp = mm(do_rows(n, 1), v_ref[n], 1, 1)
                at = lax.broadcasted_iota(jnp.int32, (BLOCK, 1), 0)
                dqi_s[n] = jnp.zeros((BLOCK, lanes), f32)
                x_s[n] = jnp.zeros((BLOCK, lanes), f32)

                def one(s, scores):
                    here = at == s
                    b_row = jnp.sum(jnp.where(here, b, 0.0), axis=0, keepdims=True)
                    k_row = jnp.sum(
                        jnp.where(here, k_ref[n].astype(f32), 0.0), axis=0, keepdims=True
                    )
                    decay = jnp.where(at >= s, jnp.exp(jnp.minimum(b - b_row, 0.0)), 0.0)
                    dp_col = jnp.sum(jnp.where(col_id == s, dp, 0.0), axis=1, keepdims=True)
                    qd = q * decay
                    column = jnp.sum(qd * k_row, axis=1, keepdims=True)
                    dq = dp_col * decay * k_row
                    dk_row = jnp.sum(dp_col * qd, axis=0, keepdims=True)
                    dqi_s[n] = dqi_s[n] + dq
                    dki_s[n] = jnp.where(here, dk_row, dki_s[n])
                    x_s[n] = x_s[n] + q * dq - jnp.where(here, dk_row * k_row, 0.0)
                    return scores + jnp.where(col_id == s, column, 0.0)

                scores = lax.fori_loop(0, BLOCK, one, jnp.zeros((BLOCK, BLOCK), f32))
                pt_s[g, BLOCK * m : BLOCK * (m + 1), BLOCK * m : BLOCK * (m + 1)] = (
                    scores.T.astype(bf16)
                )
                return carry

            lax.fori_loop(0, blocks // GROUP, within, 0)

    def spread(tensor):
        zero = jnp.zeros((BLOCK, lanes), tensor.dtype)
        return jnp.concatenate(
            [
                jnp.concatenate(
                    [tensor[m] if m == i else zero for i in range(GROUP)], axis=0
                )
                for m in range(GROUP)
            ],
            axis=1,
        )

    def forward(g, state):
        at = g * GROUP
        b = b_s[pl.ds(at, GROUP)]
        last = b[:, BLOCK - 1 :]
        grow = jnp.exp(b)
        fade = jnp.exp(last)
        qp = (q_ref[pl.ds(at, GROUP)].astype(f32) * scale * grow).astype(bf16)
        kf = (k_ref[pl.ds(at, GROUP)].astype(f32) * jnp.exp(last - b)).astype(bf16)
        qp_s[pl.ds(at, GROUP)] = qp
        kf_s[pl.ds(at, GROUP)] = kf
        v = v_ref[pl.ds(at, GROUP)].reshape(group, PAYLOAD_WIDTH)
        added = mm(v, spread(kf), 0, 0)
        do = do_rows(at, GROUP)
        for m in range(GROUP):
            n = at + m
            st_s[n] = state
            dq = mm(do[BLOCK * m : BLOCK * (m + 1)], state.astype(bf16))
            x_s[n] = x_s[n] + qp[m].astype(f32) * dq
            goes_ref[n, :BLOCK] = ((dqi_s[n] + dq * grow[m]) * scale).astype(bf16)
            state = state * fade[m] + added[:, lanes * m : lanes * (m + 1)]
        return state

    zero = jnp.zeros((PAYLOAD_WIDTH, lanes), f32)
    lax.fori_loop(0, blocks // GROUP, forward, zero, unroll=UNROLL)
    out_q = pltpu.make_async_copy(
        goes_ref.at[:, :BLOCK], goes_hbm.at[:, :BLOCK], sems.at[5]
    )
    out_q.start()

    def backward(i, dstate):
        g = blocks // GROUP - 1 - i
        at = g * GROUP
        b = b_s[pl.ds(at, GROUP)]
        last = b[:, BLOCK - 1 :]
        drop = jnp.exp(last - b)
        fade = jnp.exp(last)
        do = do_rows(at, GROUP)
        added = mm(do, spread(qp_s[pl.ds(at, GROUP)]), 0, 0)
        dv_own = mm(pt_s[g], do)
        for m in reversed(range(GROUP)):
            n = at + m
            ds = dstate.astype(bf16)
            kf = kf_s[n]
            dk = mm(v_ref[n], ds)
            goes_ref[n, BLOCK : 2 * BLOCK] = (dki_s[n] + dk * drop[m]).astype(bf16)
            dv = (dv_own[BLOCK * m : BLOCK * (m + 1)] + mm(kf, ds, 1, 1)).astype(bf16)
            for i in range(halves):
                goes_ref[n, BLOCK * (2 + i) : BLOCK * (3 + i)] = dv[
                    :, lanes * i : lanes * (i + 1)
                ]
            y_s[n] = kf.astype(f32) * dk
            e_s[n] = fade[m] * jnp.sum(st_s[n] * dstate, axis=0, keepdims=True)
            dstate = dstate * fade[m] + added[:, lanes * m : lanes * (m + 1)]
        return dstate

    lax.fori_loop(0, blocks // GROUP, backward, zero, unroll=UNROLL)
    out_kv = pltpu.make_async_copy(
        goes_ref.at[:, BLOCK : 4 * BLOCK], goes_hbm.at[:, BLOCK : 4 * BLOCK], sems.at[6]
    )
    out_kv.start()

    for n in range(blocks):
        for i, part in enumerate(three_parts(x_s[n])):
            parts[BLOCK * i : BLOCK * (i + 1), lanes * n : lanes * (n + 1)] = part
        for i, part in enumerate(three_parts(y_s[n])):
            parts[BLOCK * (3 + i) : BLOCK * (4 + i), lanes * n : lanes * (n + 1)] = part
    upper = (row_id <= col_id).astype(bf16)
    before = (row_id > col_id).astype(bf16)
    ddecay = mm(jnp.concatenate([upper] * 3 + [before] * 3, axis=1), parts[...])
    bias = jnp.zeros((1, lanes), f32)
    for n in range(blocks):
        pre = pre_s[n]
        e = jnp.exp(-jnp.abs(pre))
        slope = jnp.where(pre >= 0.0, e, 1.0) / (1.0 + e)
        gate = (
            (ddecay[:, lanes * n : lanes * (n + 1)] + e_s[n]) * slope * (1.0 / SMOOTHING)
        ).astype(bf16)
        bias = bias + jnp.sum(gate.astype(f32), axis=0, keepdims=True)
        for p in range(PACK):
            gate_s[rows * n : rows * (n + 1), lanes * p : lanes * (p + 1)] = gate[
                rows * p : rows * (p + 1)
            ]
    gates = gate_s[...]
    lowg = mm(gates, wbig[...], 1, 1)
    first = 4 * BLOCK
    goes_ref[:, first : first + rows] = lowg.reshape(blocks, rows, lanes).astype(bf16)
    cross = mm(low, gates, 0, 0)
    up = cross[:RANK, :lanes]
    for p in range(1, PACK):
        up = up + cross[RANK * p : RANK * (p + 1), lanes * p : lanes * (p + 1)]
    share = RANK // blocks
    for i, part in enumerate(two_parts(up)):
        at = first + rows + i * share
        for n in range(blocks):
            goes_ref[n, at : at + share] = part[share * n : share * (n + 1)]
    for i, part in enumerate(two_parts(bias)):
        bias_ref[i : i + 1] = part
    out_rest = pltpu.make_async_copy(
        goes_ref.at[:, first:], goes_hbm.at[:, first:], sems.at[7]
    )
    out_rest.start()
    out_bias = pltpu.make_async_copy(bias_ref, bias_hbm, sems.at[11])
    out_bias.start()
    out_bias.wait()
    out_q.wait()
    out_kv.wait()
    out_rest.wait()


def prepare_kernel(head_ref, adj_ref, wide_ref, off_ref, ex_ref, going_ref, wu_ref, offs_ref, column_ref):
    seqs, local_len, _ = adj_ref.shape
    lanes = ADDRESS_WIDTH
    pieces = PAYLOAD_WIDTH // lanes
    for b in range(seqs):
        for h in range(HEADS):
            for i in range(pieces):
                going_ref[b * HEADS + h, local_len * i : local_len * (i + 1)] = adj_ref[
                    b, :, lanes * (h * pieces + i) : lanes * (h * pieces + i + 1)
                ]
    going_ref[:, pieces * local_len :] = jnp.zeros(
        (going_ref.shape[0], going_ref.shape[1] - pieces * local_len, lanes), bf16
    )
    at = pl.multiple_of(head_ref[0] * lanes, lanes)
    wu_ref[...] = wide_ref[:, pl.ds(at, lanes)]
    offs_ref[...] = off_ref[:, pl.ds(at, lanes)]
    blocks = column_ref.shape[1]
    row_id = lax.broadcasted_iota(jnp.int32, (BLOCK, BLOCK), 0)
    col_id = lax.broadcasted_iota(jnp.int32, (BLOCK, BLOCK), 1)
    place = lax.broadcasted_iota(jnp.int32, (BLOCK, blocks), 1)
    columns = jnp.zeros((BLOCK, blocks), f32)
    for n in range(blocks):
        row = ex_ref[:, BLOCK * n : BLOCK * (n + 1)]
        column = jnp.sum(jnp.where(row_id == col_id, row, 0.0), axis=1, keepdims=True)
        columns = jnp.where(place == n, column, columns)
    column_ref[...] = columns


def prepare(head, adj, wide, off, ex):
    seqs, local_len, _ = adj.shape
    rows = PAYLOAD_WIDTH // ADDRESS_WIDTH * local_len + BLOCK // PACK
    everything = pl.BlockSpec(memory_space=pltpu.VMEM)
    return pl.pallas_call(
        prepare_kernel,
        out_shape=(
            jax.ShapeDtypeStruct((seqs * HEADS, rows, ADDRESS_WIDTH), bf16),
            jax.ShapeDtypeStruct((RANK, ADDRESS_WIDTH), bf16),
            jax.ShapeDtypeStruct((1, ADDRESS_WIDTH), f32),
            jax.ShapeDtypeStruct((BLOCK, ex.shape[1] // BLOCK), f32),
        ),
        in_specs=[pl.BlockSpec(memory_space=pltpu.SMEM)] + [everything] * 4,
        name="prepare",
    )(head.astype(jnp.int32)[None], adj, wide, off, ex)


def mixer(came, wu, off, ex, q, k, v):
    blocks = q.shape[0]
    A, V = ADDRESS_WIDTH, PAYLOAD_WIDTH
    rows = BLOCK // PACK
    height = 4 * BLOCK + rows + 2 * RANK // blocks
    vmem = pltpu.VMEM
    anywhere = pl.BlockSpec(memory_space=pl.ANY)
    return pl.pallas_call(
        mixer_kernel,
        out_shape=(
            jax.ShapeDtypeStruct((blocks, height, A), bf16),
            jax.ShapeDtypeStruct((2, A), bf16),
        ),
        in_specs=[anywhere] * 7,
        out_specs=[anywhere] * 2,
        scratch_shapes=[
            vmem((RANK, A), bf16),
            vmem((1, A), f32),
            vmem((BLOCK, blocks), f32),
            vmem((2, A), bf16),
            vmem((blocks, rows, A), bf16),
            vmem((blocks, V // A * BLOCK, A), bf16),
            vmem((blocks, BLOCK, A), bf16),
            vmem((blocks, BLOCK, A), bf16),
            vmem((blocks, BLOCK, V), bf16),
            vmem((blocks, height, A), bf16),
            vmem((A, PACK * A), bf16),
            vmem((6 * BLOCK, blocks * A), bf16),
            vmem((blocks, BLOCK, A), f32),
            vmem((blocks, BLOCK, A), f32),
            vmem((blocks, BLOCK, A), bf16),
            vmem((blocks, BLOCK, A), bf16),
            vmem((blocks, V, A), f32),
            vmem((blocks // GROUP, GROUP * BLOCK, GROUP * BLOCK), bf16),
            vmem((blocks, BLOCK, A), f32),
            vmem((blocks, BLOCK, A), f32),
            vmem((blocks, BLOCK, A), f32),
            vmem((blocks, BLOCK, A), f32),
            vmem((blocks, 1, A), f32),
            vmem((blocks * rows, PACK * A), bf16),
            pltpu.SemaphoreType.DMA((12,)),
        ],
        name="mixer",
    )(came, wu, off, ex, q, k, v)


def exchanged(tensor, axis, groups=None):
    return lax.all_to_all(
        tensor, axis, split_axis=0, concat_axis=0, tiled=True, axis_index_groups=groups
    )


def everyones(tensor, axis):
    return exchanged(jnp.broadcast_to(tensor, (lax.axis_size(axis), *tensor.shape)), axis)


def in_rows(tensor, lanes=128):
    flat = tensor.reshape(*tensor.shape[:-2], -1)
    pad = -flat.shape[-1] % lanes
    flat = jnp.pad(flat, [(0, 0)] * (flat.ndim - 1) + [(0, pad)])
    return flat.reshape(*flat.shape[:-1], -1, lanes)


def on_device(
    standardized_block_source,
    forgetting_narrowing_matrix,
    forgetting_widening_matrix,
    forgetting_offset_vector,
    probe_vectors,
    address_vectors,
    payload_vectors,
    extra_channel_forgetting,
    blender_result_adjoint,
):
    seqs, local_len, width = standardized_block_source.shape
    tokens = seqs * local_len
    length = probe_vectors.shape[1]
    blocks = length // BLOCK
    sp = lax.axis_size("sp")
    dp = lax.axis_size("dp")
    part = forgetting_narrowing_matrix.shape[0]
    A, V, R = ADDRESS_WIDTH, PAYLOAD_WIDTH, RANK
    rows = BLOCK // PACK
    contract = (((0,), (0,)), ((), ()))
    flat_input = standardized_block_source.reshape(tokens, width)

    down_rows = everyones(in_rows(forgetting_narrowing_matrix), "dp")
    down = down_rows.reshape(dp, -1)[:, : part * R].reshape(width, R)
    going, columns, offsets, extra = prepare(
        lax.axis_index("sp") % HEADS,
        blender_result_adjoint,
        forgetting_widening_matrix,
        forgetting_offset_vector[None],
        extra_channel_forgetting,
    )
    low = jnp.dot(flat_input, down, preferred_element_type=f32).astype(bf16)
    low = low.reshape(seqs, PACK, rows, R).transpose(0, 2, 1, 3).reshape(seqs, 1, rows, PACK * R)
    low = jnp.broadcast_to(low, (seqs, HEADS, rows, PACK * R)).reshape(sp, rows, A)
    going = lax.dynamic_update_slice(going, low, (0, 2 * BLOCK, 0))
    came = exchanged(going, "sp")
    goes, bias = mixer(
        came,
        columns,
        offsets,
        extra,
        probe_vectors.reshape(blocks, BLOCK, A),
        address_vectors.reshape(blocks, BLOCK, A),
        payload_vectors.reshape(blocks, BLOCK, V),
    )

    share = R // sp
    returned = exchanged(goes, "sp")
    first = returned[:, 4 * BLOCK :].astype(f32)
    low_grad = jnp.sum(first[:, :rows].reshape(seqs, HEADS, rows, A), axis=1).astype(bf16)
    low_grad = low_grad.reshape(seqs, rows, PACK, R).transpose(0, 2, 1, 3).reshape(tokens, R)
    up = first[:, rows : rows + share] + first[:, rows + share : rows + 2 * share]
    up = jnp.sum(up.reshape(seqs, HEADS, share, A), axis=0)
    up = up.transpose(1, 0, 2).reshape(share * HEADS, A)

    def to_tokens(start, pieces):
        block = returned[:, start * BLOCK : (start + pieces) * BLOCK]
        block = block.reshape(seqs, HEADS, pieces, local_len, A)
        return block.transpose(0, 3, 1, 2, 4).reshape(seqs, local_len, HEADS * pieces * A)

    grad_input = jnp.dot(low_grad, down.T, preferred_element_type=f32).astype(bf16)
    whole = lax.dot_general(flat_input, low_grad, contract, preferred_element_type=f32)
    whole = in_rows(whole.astype(bf16).reshape(dp, part, R))
    n_whole = whole.shape[1]
    own = jnp.concatenate([up.astype(bf16), bias], axis=0)
    near, far = NEAR, dp // NEAR
    near_groups = [[z * near + x for x in range(near)] for z in range(far)]
    far_groups = [[z * near + x for z in range(far)] for x in range(near)]

    def shared(pieces, rest, groups):
        count = len(groups[0])
        payload = jnp.concatenate(
            [pieces.reshape(count, -1, A), jnp.broadcast_to(rest, (count, *rest.shape))], axis=1
        )
        return jnp.sum(exchanged(payload, "dp", groups).astype(f32), axis=0)

    def bias_kept(total):
        return jnp.concatenate(
            [total[:-2].astype(bf16), *two_parts(total[-2:-1] + total[-1:])], axis=0
        )

    whole = whole.reshape(far, near, n_whole, A).transpose(1, 0, 2, 3)
    second = bias_kept(shared(whole, own, near_groups))
    second = bias_kept(
        shared(
            second[: far * n_whole].reshape(far, n_whole, A), second[far * n_whole :], far_groups
        )
    )
    third = everyones(second, "sp").astype(f32)
    down_grad = jnp.sum(third[:, :n_whole], axis=0).reshape(-1)[: part * R].reshape(part, R)
    up_grad = third[:, n_whole:-2].reshape(R, HEADS * A)
    bias_grad = jnp.sum(
        (third[:, -2] + third[:, -1]).reshape(seqs, HEADS, A), axis=0
    ).reshape(-1)
    return (
        to_tokens(0, 1),
        to_tokens(1, 1),
        to_tokens(2, 2),
        grad_input.reshape(seqs, local_len, width),
        down_grad,
        up_grad,
        bias_grad,
    )


def solution(mesh):
    placed = (
        P("dp", "sp", None),
        P("dp", None),
        P(),
        P(),
        P(("dp", "sp"), None, None),
        P(("dp", "sp"), None, None),
        P(("dp", "sp"), None, None),
        P(("dp", "sp"), None),
        P("dp", "sp", None),
    )
    return jax.shard_map(
        on_device,
        mesh=mesh,
        in_specs=placed,
        out_specs=(
            P("dp", "sp", None),
            P("dp", "sp", None),
            P("dp", "sp", None),
            P("dp", "sp", None),
            P("dp", None),
            P(),
            P(),
        ),
        check_vma=False,
    )
```

```python
import jax
import jax.numpy as jnp
from jax import lax
from jax.experimental import pallas as pl
from jax.experimental.pallas import tpu as pltpu
from jax.sharding import PartitionSpec as P

HEADS = 8
ADDRESS_WIDTH = 128
PAYLOAD_WIDTH = 256
RANK = 32
BLOCK = 64
SMOOTHING = 16.0
SPAN_LIMIT = 80.0
PACK = 4
GROUP = 4
NEAR = 4
UNROLL = 4
f32 = jnp.float32
bf16 = jnp.bfloat16


def mm(a, b, ca=1, cb=0):
    return lax.dot_general(a, b, (((ca,), (cb,)), ((), ())), preferred_element_type=f32)


def two_parts(a):
    hi = a.astype(bf16)
    return hi, (a - hi.astype(f32)).astype(bf16)


def three_parts(a):
    hi = a.astype(bf16)
    return hi, *two_parts(a - hi.astype(f32))


def mixer_kernel(
    came_hbm, wu_hbm, off_hbm, ex_hbm, q_hbm, k_hbm, v_hbm,
    goes_hbm, bias_hbm,
    wu_ref, off_ref, ex_ref, bias_ref, low_s, do_ref, q_ref, k_ref, v_ref, goes_ref, wbig, parts, b_s, pre_s, qp_s, kf_s, st_s,
    pt_s, dqi_s, dki_s, x_s, e_s, gate_s, sems,
):
    blocks = q_ref.shape[0]
    rows = BLOCK // PACK
    lanes = ADDRESS_WIDTH
    scale = ADDRESS_WIDTH ** (-0.5)
    middle = BLOCK // 2
    group = GROUP * BLOCK
    halves = PAYLOAD_WIDTH // lanes

    copies = [
        pltpu.make_async_copy(came_hbm.at[:, halves * BLOCK :], low_s, sems.at[0]),
        pltpu.make_async_copy(wu_hbm, wu_ref, sems.at[8]),
        pltpu.make_async_copy(off_hbm, off_ref, sems.at[9]),
        pltpu.make_async_copy(ex_hbm, ex_ref, sems.at[10]),
        pltpu.make_async_copy(q_hbm, q_ref, sems.at[1]),
        pltpu.make_async_copy(k_hbm, k_ref, sems.at[2]),
        pltpu.make_async_copy(came_hbm.at[:, : halves * BLOCK], do_ref, sems.at[3]),
        pltpu.make_async_copy(v_hbm, v_ref, sems.at[4]),
    ]
    for copy in copies:
        copy.start()

    def do_rows(at, count):
        both = do_ref[pl.ds(at, count)]
        return jnp.concatenate(
            [
                both[:, BLOCK * i : BLOCK * (i + 1)].reshape(count * BLOCK, lanes)
                for i in range(halves)
            ],
            axis=1,
        )

    row_id = lax.broadcasted_iota(jnp.int32, (BLOCK, BLOCK), 0)
    col_id = lax.broadcasted_iota(jnp.int32, (BLOCK, BLOCK), 1)

    wbig[...] = jnp.zeros(wbig.shape, bf16)
    for copy in copies[:4]:
        copy.wait()
    for p in range(PACK):
        wbig[RANK * p : RANK * (p + 1), lanes * p : lanes * (p + 1)] = wu_ref[...]
    low = low_s[...].reshape(blocks * rows, lanes)
    raw = mm(low, wbig[...])
    offs = off_ref[...]
    for n in range(blocks):
        pre = (
            jnp.concatenate(
                [
                    raw[rows * n : rows * (n + 1), lanes * p : lanes * (p + 1)]
                    for p in range(PACK)
                ],
                axis=0,
            )
            + offs
        )
        pre_s[n] = pre
        decay = (jnp.minimum(pre, 0.0) - jnp.log1p(jnp.exp(-jnp.abs(pre)))) * (
            1.0 / SMOOTHING
        ) + ex_ref[:, n : n + 1]
        for i, part in enumerate(three_parts(decay)):
            parts[BLOCK * i : BLOCK * (i + 1), lanes * n : lanes * (n + 1)] = part
    lower = (row_id >= col_id).astype(bf16)
    sums = mm(jnp.concatenate([lower] * 3, axis=1), parts[: 3 * BLOCK])
    span = jnp.zeros((1, lanes), f32)
    for n in range(blocks):
        b = sums[:, lanes * n : lanes * (n + 1)]
        b_s[n] = b
        centre = b[middle : middle + 1]
        span = jnp.maximum(span, jnp.maximum(b[:1] - centre, centre - b[BLOCK - 1 :]))
    narrow = jnp.max(span) < SPAN_LIMIT
    for copy in copies[4:]:
        copy.wait()

    @pl.when(narrow)
    def _():
        big_row = lax.broadcasted_iota(jnp.int32, (group, group), 0)
        big_col = lax.broadcasted_iota(jnp.int32, (group, group), 1)
        same = big_row // BLOCK == big_col // BLOCK
        causal = same & (big_row >= big_col)
        mirrored = same & (big_row <= big_col)

        def within(g, carry):
            at = g * GROUP
            b = b_s[pl.ds(at, GROUP)]
            centre = b[:, middle : middle + 1]
            lift = jnp.exp(b - centre).reshape(group, lanes)
            drop = jnp.exp(centre - b).reshape(group, lanes)
            q = q_ref[pl.ds(at, GROUP)].astype(f32).reshape(group, lanes)
            k = k_ref[pl.ds(at, GROUP)].astype(f32).reshape(group, lanes)
            qc = (q * scale * lift).astype(bf16)
            kc = (k * drop).astype(bf16)
            do = do_rows(at, GROUP)
            v = v_ref[pl.ds(at, GROUP)].reshape(group, PAYLOAD_WIDTH)
            pt_s[g] = jnp.where(mirrored, mm(kc, qc, 1, 1), 0.0).astype(bf16)
            dp = jnp.where(causal, mm(do, v, 1, 1), 0.0).astype(bf16)
            dq = mm(dp, kc)
            dk = mm(dp, qc, 0, 0)
            shape = (GROUP, BLOCK, lanes)
            x_s[pl.ds(at, GROUP)] = (dq * qc.astype(f32) - dk * kc.astype(f32)).reshape(shape)
            dqi_s[pl.ds(at, GROUP)] = (dq * lift).reshape(shape)
            dki_s[pl.ds(at, GROUP)] = (dk * drop).reshape(shape)
            return carry

        lax.fori_loop(0, blocks // GROUP, within, 0, unroll=UNROLL)

    @pl.when(jnp.logical_not(narrow))
    def _():
        pt_s[...] = jnp.zeros(pt_s.shape, bf16)
        for m in range(GROUP):
            def within(g, carry, m=m):
                n = g * GROUP + m
                b = b_s[n]
                q = q_ref[n].astype(f32) * scale
                dp = mm(do_rows(n, 1), v_ref[n], 1, 1)
                at = lax.broadcasted_iota(jnp.int32, (BLOCK, 1), 0)
                dqi_s[n] = jnp.zeros((BLOCK, lanes), f32)
                x_s[n] = jnp.zeros((BLOCK, lanes), f32)

                def one(s, scores):
                    here = at == s
                    b_row = jnp.sum(jnp.where(here, b, 0.0), axis=0, keepdims=True)
                    k_row = jnp.sum(
                        jnp.where(here, k_ref[n].astype(f32), 0.0), axis=0, keepdims=True
                    )
                    decay = jnp.where(at >= s, jnp.exp(jnp.minimum(b - b_row, 0.0)), 0.0)
                    dp_col = jnp.sum(jnp.where(col_id == s, dp, 0.0), axis=1, keepdims=True)
                    qd = q * decay
                    column = jnp.sum(qd * k_row, axis=1, keepdims=True)
                    dq = dp_col * decay * k_row
                    dk_row = jnp.sum(dp_col * qd, axis=0, keepdims=True)
                    dqi_s[n] = dqi_s[n] + dq
                    dki_s[n] = jnp.where(here, dk_row, dki_s[n])
                    x_s[n] = x_s[n] + q * dq - jnp.where(here, dk_row * k_row, 0.0)
                    return scores + jnp.where(col_id == s, column, 0.0)

                scores = lax.fori_loop(0, BLOCK, one, jnp.zeros((BLOCK, BLOCK), f32))
                pt_s[g, BLOCK * m : BLOCK * (m + 1), BLOCK * m : BLOCK * (m + 1)] = (
                    scores.T.astype(bf16)
                )
                return carry

            lax.fori_loop(0, blocks // GROUP, within, 0)

    def split(n, first, terms):
        for i, part in enumerate(three_parts(terms), first):
            parts[BLOCK * i : BLOCK * (i + 1), lanes * n : lanes * (n + 1)] = part

    def spread(tensor):
        zero = jnp.zeros((BLOCK, lanes), tensor.dtype)
        return jnp.concatenate(
            [
                jnp.concatenate(
                    [tensor[m] if m == i else zero for i in range(GROUP)], axis=0
                )
                for m in range(GROUP)
            ],
            axis=1,
        )

    def forward(g, state):
        at = g * GROUP
        b = b_s[pl.ds(at, GROUP)]
        last = b[:, BLOCK - 1 :]
        grow = jnp.exp(b)
        fade = jnp.exp(last)
        qp = (q_ref[pl.ds(at, GROUP)].astype(f32) * scale * grow).astype(bf16)
        kf = (k_ref[pl.ds(at, GROUP)].astype(f32) * jnp.exp(last - b)).astype(bf16)
        qp_s[pl.ds(at, GROUP)] = qp
        kf_s[pl.ds(at, GROUP)] = kf
        v = v_ref[pl.ds(at, GROUP)].reshape(group, PAYLOAD_WIDTH)
        added = mm(v, spread(kf), 0, 0)
        do = do_rows(at, GROUP)
        for m in range(GROUP):
            n = at + m
            st_s[n] = state
            dq = mm(do[BLOCK * m : BLOCK * (m + 1)], state.astype(bf16))
            split(n, 0, x_s[n] + qp[m].astype(f32) * dq)
            pre = pre_s[n]
            e = jnp.exp(-jnp.abs(pre))
            pre_s[n] = jnp.where(pre >= 0.0, e, 1.0) / (1.0 + e)
            goes_ref[n, :BLOCK] = ((dqi_s[n] + dq * grow[m]) * scale).astype(bf16)
            state = state * fade[m] + added[:, lanes * m : lanes * (m + 1)]
        return state

    zero = jnp.zeros((PAYLOAD_WIDTH, lanes), f32)
    state = zero
    for g in range(blocks // GROUP):
        state = forward(g, state)
    out_q = pltpu.make_async_copy(
        goes_ref.at[:, :BLOCK], goes_hbm.at[:, :BLOCK], sems.at[5]
    )
    out_q.start()

    def backward(i, dstate):
        g = blocks // GROUP - 1 - i
        at = g * GROUP
        b = b_s[pl.ds(at, GROUP)]
        last = b[:, BLOCK - 1 :]
        drop = jnp.exp(last - b)
        fade = jnp.exp(last)
        do = do_rows(at, GROUP)
        added = mm(do, spread(qp_s[pl.ds(at, GROUP)]), 0, 0)
        dv_own = mm(pt_s[g], do)
        for m in reversed(range(GROUP)):
            n = at + m
            ds = dstate.astype(bf16)
            kf = kf_s[n]
            dk = mm(v_ref[n], ds)
            goes_ref[n, BLOCK : 2 * BLOCK] = (dki_s[n] + dk * drop[m]).astype(bf16)
            dv = (dv_own[BLOCK * m : BLOCK * (m + 1)] + mm(kf, ds, 1, 1)).astype(bf16)
            for i in range(halves):
                goes_ref[n, BLOCK * (2 + i) : BLOCK * (3 + i)] = dv[
                    :, lanes * i : lanes * (i + 1)
                ]
            split(n, 3, kf.astype(f32) * dk)
            e_s[n] = fade[m] * jnp.sum(st_s[n] * dstate, axis=0, keepdims=True)
            dstate = dstate * fade[m] + added[:, lanes * m : lanes * (m + 1)]
        return dstate

    dstate = zero
    for i in range(blocks // GROUP):
        dstate = backward(i, dstate)
    out_kv = pltpu.make_async_copy(
        goes_ref.at[:, BLOCK : 4 * BLOCK], goes_hbm.at[:, BLOCK : 4 * BLOCK], sems.at[6]
    )
    out_kv.start()

    upper = (row_id <= col_id).astype(bf16)
    before = (row_id > col_id).astype(bf16)
    ddecay = mm(jnp.concatenate([upper] * 3 + [before] * 3, axis=1), parts[...])
    bias = jnp.zeros((1, lanes), f32)
    for n in range(blocks):
        gate = (
            (ddecay[:, lanes * n : lanes * (n + 1)] + e_s[n]) * pre_s[n] * (1.0 / SMOOTHING)
        ).astype(bf16)
        bias = bias + jnp.sum(gate.astype(f32), axis=0, keepdims=True)
        for p in range(PACK):
            gate_s[rows * n : rows * (n + 1), lanes * p : lanes * (p + 1)] = gate[
                rows * p : rows * (p + 1)
            ]
    gates = gate_s[...]
    lowg = mm(gates, wbig[...], 1, 1)
    first = 4 * BLOCK
    goes_ref[:, first : first + rows] = lowg.reshape(blocks, rows, lanes).astype(bf16)
    cross = mm(low, gates, 0, 0)
    up = cross[:RANK, :lanes]
    for p in range(1, PACK):
        up = up + cross[RANK * p : RANK * (p + 1), lanes * p : lanes * (p + 1)]
    share = RANK // blocks
    for i, part in enumerate(two_parts(up)):
        at = first + rows + i * share
        for n in range(blocks):
            goes_ref[n, at : at + share] = part[share * n : share * (n + 1)]
    for i, part in enumerate(two_parts(bias)):
        bias_ref[i : i + 1] = part
    out_rest = pltpu.make_async_copy(
        goes_ref.at[:, first:], goes_hbm.at[:, first:], sems.at[7]
    )
    out_rest.start()
    out_bias = pltpu.make_async_copy(bias_ref, bias_hbm, sems.at[11])
    out_bias.start()
    out_bias.wait()
    out_q.wait()
    out_kv.wait()
    out_rest.wait()


def prepare_kernel(head_ref, adj_ref, wide_ref, off_ref, ex_ref, going_ref, wu_ref, offs_ref, column_ref):
    seqs, local_len, _ = adj_ref.shape
    lanes = ADDRESS_WIDTH
    pieces = PAYLOAD_WIDTH // lanes
    for b in range(seqs):
        for h in range(HEADS):
            for i in range(pieces):
                going_ref[b * HEADS + h, local_len * i : local_len * (i + 1)] = adj_ref[
                    b, :, lanes * (h * pieces + i) : lanes * (h * pieces + i + 1)
                ]
    going_ref[:, pieces * local_len :] = jnp.zeros(
        (going_ref.shape[0], going_ref.shape[1] - pieces * local_len, lanes), bf16
    )
    at = pl.multiple_of(head_ref[0] * lanes, lanes)
    wu_ref[...] = wide_ref[:, pl.ds(at, lanes)]
    offs_ref[...] = off_ref[:, pl.ds(at, lanes)]
    blocks = column_ref.shape[1]
    row_id = lax.broadcasted_iota(jnp.int32, (BLOCK, BLOCK), 0)
    col_id = lax.broadcasted_iota(jnp.int32, (BLOCK, BLOCK), 1)
    place = lax.broadcasted_iota(jnp.int32, (BLOCK, blocks), 1)
    columns = jnp.zeros((BLOCK, blocks), f32)
    for n in range(blocks):
        row = ex_ref[:, BLOCK * n : BLOCK * (n + 1)]
        column = jnp.sum(jnp.where(row_id == col_id, row, 0.0), axis=1, keepdims=True)
        columns = jnp.where(place == n, column, columns)
    column_ref[...] = columns


def prepare(head, adj, wide, off, ex):
    seqs, local_len, _ = adj.shape
    rows = PAYLOAD_WIDTH // ADDRESS_WIDTH * local_len + BLOCK // PACK
    everything = pl.BlockSpec(memory_space=pltpu.VMEM)
    return pl.pallas_call(
        prepare_kernel,
        out_shape=(
            jax.ShapeDtypeStruct((seqs * HEADS, rows, ADDRESS_WIDTH), bf16),
            jax.ShapeDtypeStruct((RANK, ADDRESS_WIDTH), bf16),
            jax.ShapeDtypeStruct((1, ADDRESS_WIDTH), f32),
            jax.ShapeDtypeStruct((BLOCK, ex.shape[1] // BLOCK), f32),
        ),
        in_specs=[pl.BlockSpec(memory_space=pltpu.SMEM)] + [everything] * 4,
        name="prepare",
    )(head.astype(jnp.int32)[None], adj, wide, off, ex)


def mixer(came, wu, off, ex, q, k, v):
    blocks = q.shape[0]
    A, V = ADDRESS_WIDTH, PAYLOAD_WIDTH
    rows = BLOCK // PACK
    height = 4 * BLOCK + rows + 2 * RANK // blocks
    vmem = pltpu.VMEM
    anywhere = pl.BlockSpec(memory_space=pl.ANY)
    return pl.pallas_call(
        mixer_kernel,
        out_shape=(
            jax.ShapeDtypeStruct((blocks, height, A), bf16),
            jax.ShapeDtypeStruct((2, A), bf16),
        ),
        in_specs=[anywhere] * 7,
        out_specs=[anywhere] * 2,
        scratch_shapes=[
            vmem((RANK, A), bf16),
            vmem((1, A), f32),
            vmem((BLOCK, blocks), f32),
            vmem((2, A), bf16),
            vmem((blocks, rows, A), bf16),
            vmem((blocks, V // A * BLOCK, A), bf16),
            vmem((blocks, BLOCK, A), bf16),
            vmem((blocks, BLOCK, A), bf16),
            vmem((blocks, BLOCK, V), bf16),
            vmem((blocks, height, A), bf16),
            vmem((A, PACK * A), bf16),
            vmem((6 * BLOCK, blocks * A), bf16),
            vmem((blocks, BLOCK, A), f32),
            vmem((blocks, BLOCK, A), f32),
            vmem((blocks, BLOCK, A), bf16),
            vmem((blocks, BLOCK, A), bf16),
            vmem((blocks, V, A), f32),
            vmem((blocks // GROUP, GROUP * BLOCK, GROUP * BLOCK), bf16),
            vmem((blocks, BLOCK, A), f32),
            vmem((blocks, BLOCK, A), f32),
            vmem((blocks, BLOCK, A), f32),
            vmem((blocks, 1, A), f32),
            vmem((blocks * rows, PACK * A), bf16),
            pltpu.SemaphoreType.DMA((12,)),
        ],
        name="mixer",
    )(came, wu, off, ex, q, k, v)


def exchanged(tensor, axis, groups=None):
    return lax.all_to_all(
        tensor, axis, split_axis=0, concat_axis=0, tiled=True, axis_index_groups=groups
    )


def everyones(tensor, axis):
    return exchanged(jnp.broadcast_to(tensor, (lax.axis_size(axis), *tensor.shape)), axis)


def in_rows(tensor, lanes=128):
    flat = tensor.reshape(*tensor.shape[:-2], -1)
    pad = -flat.shape[-1] % lanes
    flat = jnp.pad(flat, [(0, 0)] * (flat.ndim - 1) + [(0, pad)])
    return flat.reshape(*flat.shape[:-1], -1, lanes)


def on_device(
    standardized_block_source,
    forgetting_narrowing_matrix,
    forgetting_widening_matrix,
    forgetting_offset_vector,
    probe_vectors,
    address_vectors,
    payload_vectors,
    extra_channel_forgetting,
    blender_result_adjoint,
):
    seqs, local_len, width = standardized_block_source.shape
    tokens = seqs * local_len
    length = probe_vectors.shape[1]
    blocks = length // BLOCK
    sp = lax.axis_size("sp")
    dp = lax.axis_size("dp")
    part = forgetting_narrowing_matrix.shape[0]
    A, V, R = ADDRESS_WIDTH, PAYLOAD_WIDTH, RANK
    rows = BLOCK // PACK
    contract = (((0,), (0,)), ((), ()))
    flat_input = standardized_block_source.reshape(tokens, width)

    down_rows = everyones(in_rows(forgetting_narrowing_matrix), "dp")
    down = down_rows.reshape(dp, -1)[:, : part * R].reshape(width, R)
    going, columns, offsets, extra = prepare(
        lax.axis_index("sp") % HEADS,
        blender_result_adjoint,
        forgetting_widening_matrix,
        forgetting_offset_vector[None],
        extra_channel_forgetting,
    )
    low = jnp.dot(flat_input, down, preferred_element_type=f32).astype(bf16)
    low = low.reshape(seqs, PACK, rows, R).transpose(0, 2, 1, 3).reshape(seqs, 1, rows, PACK * R)
    low = jnp.broadcast_to(low, (seqs, HEADS, rows, PACK * R)).reshape(sp, rows, A)
    going = lax.dynamic_update_slice(going, low, (0, 2 * BLOCK, 0))
    came = exchanged(going, "sp")
    goes, bias = mixer(
        came,
        columns,
        offsets,
        extra,
        probe_vectors.reshape(blocks, BLOCK, A),
        address_vectors.reshape(blocks, BLOCK, A),
        payload_vectors.reshape(blocks, BLOCK, V),
    )

    share = R // sp
    returned = exchanged(goes, "sp")
    first = returned[:, 4 * BLOCK :].astype(f32)
    low_grad = jnp.sum(first[:, :rows].reshape(seqs, HEADS, rows, A), axis=1).astype(bf16)
    low_grad = low_grad.reshape(seqs, rows, PACK, R).transpose(0, 2, 1, 3).reshape(tokens, R)
    up = first[:, rows : rows + share] + first[:, rows + share : rows + 2 * share]
    up = jnp.sum(up.reshape(seqs, HEADS, share, A), axis=0)
    up = up.transpose(1, 0, 2).reshape(share * HEADS, A)

    def to_tokens(start, pieces):
        block = returned[:, start * BLOCK : (start + pieces) * BLOCK]
        block = block.reshape(seqs, HEADS, pieces, local_len, A)
        return block.transpose(0, 3, 1, 2, 4).reshape(seqs, local_len, HEADS * pieces * A)

    grad_input = jnp.dot(low_grad, down.T, preferred_element_type=f32).astype(bf16)
    whole = lax.dot_general(flat_input, low_grad, contract, preferred_element_type=f32)
    whole = in_rows(whole.astype(bf16).reshape(dp, part, R))
    n_whole = whole.shape[1]
    own = jnp.concatenate([up.astype(bf16), bias], axis=0)
    near, far = NEAR, dp // NEAR
    near_groups = [[z * near + x for x in range(near)] for z in range(far)]
    far_groups = [[z * near + x for z in range(far)] for x in range(near)]

    def shared(pieces, rest, groups):
        count = len(groups[0])
        payload = jnp.concatenate(
            [pieces.reshape(count, -1, A), jnp.broadcast_to(rest, (count, *rest.shape))], axis=1
        )
        return jnp.sum(exchanged(payload, "dp", groups).astype(f32), axis=0)

    def bias_kept(total):
        return jnp.concatenate(
            [total[:-2].astype(bf16), *two_parts(total[-2:-1] + total[-1:])], axis=0
        )

    whole = whole.reshape(far, near, n_whole, A).transpose(1, 0, 2, 3)
    second = bias_kept(shared(whole, own, near_groups))
    second = bias_kept(
        shared(
            second[: far * n_whole].reshape(far, n_whole, A), second[far * n_whole :], far_groups
        )
    )
    third = everyones(second, "sp").astype(f32)
    down_grad = jnp.sum(third[:, :n_whole], axis=0).reshape(-1)[: part * R].reshape(part, R)
    up_grad = third[:, n_whole:-2].reshape(R, HEADS * A)
    bias_grad = jnp.sum(
        (third[:, -2] + third[:, -1]).reshape(seqs, HEADS, A), axis=0
    ).reshape(-1)
    return (
        to_tokens(0, 1),
        to_tokens(1, 1),
        to_tokens(2, 2),
        grad_input.reshape(seqs, local_len, width),
        down_grad,
        up_grad,
        bias_grad,
    )


def solution(mesh):
    placed = (
        P("dp", "sp", None),
        P("dp", None),
        P(),
        P(),
        P(("dp", "sp"), None, None),
        P(("dp", "sp"), None, None),
        P(("dp", "sp"), None, None),
        P(("dp", "sp"), None),
        P("dp", "sp", None),
    )
    return jax.shard_map(
        on_device,
        mesh=mesh,
        in_specs=placed,
        out_specs=(
            P("dp", "sp", None),
            P("dp", "sp", None),
            P("dp", "sp", None),
            P("dp", "sp", None),
            P("dp", None),
            P(),
            P(),
        ),
        check_vma=False,
    )
```
